32 devices in a mesh: sp: 4 (over z), dp: 8 (over y, x, core).
Axes of the slice: x: 2, y: 2, z: 4, core: 2. Of those that a mesh axis runs over, the one named last changes fastest.
Arguments:
- inputs: bfloat16 [8, 512, 2048], P('dp', 'sp'), may hold values from -0.75 to 0.75
- queries: bfloat16 [8, 512, 1024], P('dp', 'sp'), may hold values from -18 to 18
- keys: bfloat16 [8, 512, 256], P('dp', 'sp'), may hold values from -18 to 18
- values: bfloat16 [8, 512, 256], P('dp', 'sp'), may hold values from -6 to 6
- out_grad: bfloat16 [8, 512, 1024], P('dp', 'sp'), may hold values from -144 to 144
- query_gain: float32 [64], replicated, may hold values from 0.4 to 6.5
- key_gain: float32 [64], replicated, may hold values from 0.4 to 6.5
- key_matrix: bfloat16 [2048, 256], P('dp'), may hold values from -0.125 to 0.125
- value_matrix: bfloat16 [2048, 256], P('dp'), may hold values from -0.125 to 0.125
Outputs:
- input_grad: bfloat16 [8, 512, 2048], P('dp', 'sp')
- query_grad: bfloat16 [8, 512, 1024], P('dp', 'sp')
- key_weight_grad: float32 [2048, 256], P('dp')
- value_weight_grad: float32 [2048, 256], P('dp')
The draws below stay inside these ranges and needn't reach their ends.
All inputs are finite; a program needn't handle non-finite values.
Results may differ from the reference program's by a relative error of at most 0.024.
The reference program's roundings to bfloat16 on the way count: a program that leaves them out, or rounds other values in their place, can miss the bound.
Values may be sent and summed in bfloat16 or wider, within the bound.
A program may use at most 64 MiB of HBM per device.

```python
import jax
import jax.numpy as jnp
from jax import lax

MODEL_WIDTH = 2048
QUERY_HEADS = 16
KEY_VALUE_HEADS = 4
HEAD_CHANNELS = 64
GRID = 64
SEQUENCE_LENGTH = 512
SEQUENCE_COUNT = 8
HPART = 4


def gain_draw(seed_key):
    return jnp.clip(1.0 + 0.18 * jax.random.normal(seed_key, (HEAD_CHANNELS,), jnp.float32), 0.4, 1.6)


def draw_query_gain(key, part):
    return gain_draw(jax.random.fold_in(key, 11))


def draw_key_gain(key, part):
    return gain_draw(jax.random.fold_in(key, 23))


def level_of(stream_key, extent, cuts, low, largest):
    def one(dim, parts):
        steps = jax.random.uniform(jax.random.fold_in(jax.random.fold_in(stream_key, 6), dim), (parts,), jnp.float32, low / len(cuts), largest / len(cuts))
        return jnp.repeat(jnp.exp(steps), extent[dim] // parts).reshape((-1,) + (1,) * (len(extent) - dim - 1))

    level = one(*cuts[0])
    for cut in cuts[1:]:
        level = level * one(*cut)
    return level


def bell_draw(rng, shape, deviation, limit, shards=(), kind=jnp.bfloat16):
    entries = jax.random.normal(rng, shape, jnp.float32) * deviation
    if len(shards) > 0:
        entries = level_of(rng, shape, shards, -0.22, 0.18) * entries
    return jnp.clip(entries, min=-limit, max=limit).astype(kind)


def setup_inputs(seed: int = 0) -> dict:
    arg_keys = jax.random.split(jax.random.key(seed), 10)
    return {
        "inputs": bell_draw(arg_keys[0], (SEQUENCE_COUNT, SEQUENCE_LENGTH, MODEL_WIDTH), 0.125, 0.75, ((0, 8), (1, 4))),
        "queries": bell_draw(arg_keys[1], (SEQUENCE_COUNT, SEQUENCE_LENGTH, QUERY_HEADS * HEAD_CHANNELS), 3.0, 18.0, ((0, 8), (1, 4))),
        "keys": bell_draw(arg_keys[2], (SEQUENCE_COUNT, SEQUENCE_LENGTH, KEY_VALUE_HEADS * HEAD_CHANNELS), 3.0, 18.0, ((0, 8), (1, 4))),
        "values": bell_draw(arg_keys[3], (SEQUENCE_COUNT, SEQUENCE_LENGTH, KEY_VALUE_HEADS * HEAD_CHANNELS), 1.0, 6.0, ((0, 8), (1, 4))),
        "out_grad": bell_draw(arg_keys[4], (SEQUENCE_COUNT, SEQUENCE_LENGTH, QUERY_HEADS * HEAD_CHANNELS), 24.0, 144.0, ((0, 8), (1, 4))),
        "query_gain": draw_query_gain(jax.random.fold_in(arg_keys[9], 71), 0),
        "key_gain": draw_key_gain(jax.random.fold_in(arg_keys[9], 71), 0),
        "key_matrix": bell_draw(arg_keys[7], (MODEL_WIDTH, KEY_VALUE_HEADS * HEAD_CHANNELS), MODEL_WIDTH ** -0.5, 0.125, ((0, 8),)),
        "value_matrix": bell_draw(arg_keys[8], (MODEL_WIDTH, KEY_VALUE_HEADS * HEAD_CHANNELS), MODEL_WIDTH ** -0.5, 0.125, ((0, 8),)),
    }


rope_base = 10000.0
norm_eps = 0.5
score_scale = 0.125

def product(pattern, first_op, second_op):
    return jnp.einsum(pattern, first_op.astype(jnp.float32), second_op.astype(jnp.float32))

def rotary_tables(token_length):
    position = jnp.arange(token_length, dtype=jnp.int32)
    grid_row = (position // GRID).astype(jnp.float32)
    grid_col = (position % GRID).astype(jnp.float32)
    half_pairs = HEAD_CHANNELS // 4
    inv_freq = rope_base ** (-jnp.arange(half_pairs, dtype=jnp.float32) / half_pairs)
    angles = jnp.concatenate([grid_row[:, None] * inv_freq, grid_col[:, None] * inv_freq], axis=1)
    return (jnp.cos(angles), jnp.sin(angles))

def rotate(vector, cos_tab, sin_tab):
    even_part = vector[..., 0::2]
    odd_part = vector[..., 1::2]
    turned = jnp.stack([even_part * cos_tab - odd_part * sin_tab, even_part * sin_tab + odd_part * cos_tab], axis=-1)
    return turned.reshape(vector.shape)

def rotate_back(cotangent, cos_tab, sin_tab):
    even_part = cotangent[..., 0::2]
    odd_part = cotangent[..., 1::2]
    turned = jnp.stack([even_part * cos_tab + odd_part * sin_tab, odd_part * cos_tab - even_part * sin_tab], axis=-1)
    return turned.reshape(cotangent.shape)

def inverse_rms(vector):
    return lax.rsqrt(lax.optimization_barrier(jnp.mean(vector * vector, axis=-1, keepdims=True)) + norm_eps)

def norm_back(vector, inv_scale, cotangent, gain_vec):
    weighted = cotangent * gain_vec
    inner_mean = lax.optimization_barrier(jnp.mean(weighted * vector, axis=-1, keepdims=True))
    return inv_scale * (weighted - vector * inv_scale * inv_scale * inner_mean)

def head_grads(query_in, key_input, value_input, grad_in, query_gain, key_gain, cos_tab, sin_tab, block_rows):
    token_length, groups, per_group, head_dim = query_in.shape
    cos_four = cos_tab[:, None, None, :]
    sin_four = sin_tab[:, None, None, :]
    cos_three = cos_tab[:, None, :]
    sin_three = sin_tab[:, None, :]
    query_f = query_in.astype(jnp.float32)
    query_inv = inverse_rms(query_f)
    query_rot = rotate(query_f * query_inv * query_gain, cos_four, sin_four).astype(jnp.bfloat16)
    key_f = key_input.astype(jnp.float32)
    key_inv = inverse_rms(key_f)
    key_rot = rotate(key_f * key_inv * key_gain, cos_three, sin_three).astype(jnp.bfloat16)
    num_blocks = token_length // block_rows
    query_blocks = query_rot.reshape(num_blocks, block_rows, groups, per_group, head_dim)
    grad_blocks = grad_in.reshape(num_blocks, block_rows, groups, per_group, head_dim)

    def attend_block(carried, pieces):
        key_acc, value_acc = carried
        query_piece, grad_piece = pieces
        scores = product('qgrd,cgd->grqc', query_piece, key_rot) * score_scale
        row_max = lax.optimization_barrier(jnp.max(scores, axis=-1, keepdims=True))
        shifted = jnp.exp(scores - row_max)
        attn_prob = shifted / lax.optimization_barrier(jnp.sum(shifted, axis=-1, keepdims=True))
        prob_low = attn_prob.astype(jnp.bfloat16)
        prob_grad = product('qgrd,cgd->grqc', grad_piece, value_input)
        row_dot = lax.optimization_barrier(jnp.sum(attn_prob * prob_grad, axis=-1, keepdims=True))
        score_grad = (attn_prob * (prob_grad - row_dot) * score_scale).astype(jnp.bfloat16)
        dq_piece = product('grqc,cgd->qgrd', score_grad, key_rot)
        key_acc = key_acc + product('grqc,qgrd->cgd', score_grad, query_piece)
        value_acc = value_acc + product('grqc,qgrd->cgd', prob_low, grad_piece)
        return ((key_acc, value_acc), dq_piece)
    empty_acc = jnp.zeros((token_length, groups, head_dim), jnp.float32)
    (key_rot_grad, value_acc), query_rot_grad = lax.scan(attend_block, (empty_acc, empty_acc), (query_blocks, grad_blocks))
    query_rot_grad = query_rot_grad.reshape(token_length, groups, per_group, head_dim)
    query_grad = norm_back(query_f, query_inv, rotate_back(query_rot_grad, cos_four, sin_four), query_gain).astype(jnp.bfloat16)
    key_portion = norm_back(key_f, key_inv, rotate_back(key_rot_grad, cos_three, sin_three), key_gain).astype(jnp.bfloat16)
    return (query_grad, key_portion, value_acc.astype(jnp.bfloat16))

def reference(inputs, queries, keys, values, out_grad, query_gain, key_gain, key_matrix, value_matrix):
    token_length = queries.shape[1]
    portion_count = QUERY_HEADS // HPART
    group_copies = portion_count // KEY_VALUE_HEADS
    cos_tab, sin_tab = rotary_tables(token_length)
    block_rows = min(512, token_length)

    def sequence_grads(pack):
        query_in, key_input, value_input, grad_in = pack
        key_positions = jnp.repeat(key_input.reshape(token_length, KEY_VALUE_HEADS, HEAD_CHANNELS), group_copies, axis=1)
        value_positions = jnp.repeat(value_input.reshape(token_length, KEY_VALUE_HEADS, HEAD_CHANNELS), group_copies, axis=1)
        query_part, key_portion, value_portion = head_grads(query_in.reshape(token_length, portion_count, HPART, HEAD_CHANNELS), key_positions, value_positions, grad_in.reshape(token_length, portion_count, HPART, HEAD_CHANNELS), query_gain, key_gain, cos_tab, sin_tab, block_rows)
        key_gradient = key_portion.reshape(token_length, KEY_VALUE_HEADS, group_copies, HEAD_CHANNELS).astype(jnp.float32).sum(axis=2).astype(jnp.bfloat16)
        value_gradient = value_portion.reshape(token_length, KEY_VALUE_HEADS, group_copies, HEAD_CHANNELS).astype(jnp.float32).sum(axis=2).astype(jnp.bfloat16)
        joined_output = jnp.concatenate([key_gradient.reshape(token_length, KEY_VALUE_HEADS * HEAD_CHANNELS), value_gradient.reshape(token_length, KEY_VALUE_HEADS * HEAD_CHANNELS)], axis=1)
        return (query_part.reshape(token_length, QUERY_HEADS * HEAD_CHANNELS), joined_output)
    query_grad, projection_gradient = lax.map(sequence_grads, (queries, keys, values, out_grad))
    joined_weight = jnp.concatenate([key_matrix, value_matrix], axis=1)
    flattened_gradient = projection_gradient.reshape(-1, 2 * KEY_VALUE_HEADS * HEAD_CHANNELS)
    input_grad = jnp.dot(flattened_gradient, joined_weight.T, preferred_element_type=jnp.float32).astype(jnp.bfloat16)
    input_grad = input_grad.reshape(inputs.shape)
    weight_grad = jnp.dot(inputs.reshape(-1, inputs.shape[2]).T, flattened_gradient, preferred_element_type=jnp.float32)
    key_value_width = KEY_VALUE_HEADS * HEAD_CHANNELS
    return (input_grad, query_grad, weight_grad[:, :key_value_width], weight_grad[:, key_value_width:])
```

```python
import functools

import jax
import jax.numpy as jnp
import numpy as np
from jax import lax
from jax.experimental import pallas as pl
from jax.experimental.pallas import tpu as pltpu
from jax.sharding import PartitionSpec as P

QUERY_HEADS = 16
KEY_VALUE_HEADS = 4
HEAD_CHANNELS = 64
GRID = 64


rope_base = 10000.0
norm_eps = 0.5
score_scale = 0.125


def product(pattern, first_op, second_op):
    return jnp.einsum(pattern, first_op, second_op, preferred_element_type=jnp.float32)


def rotary_tables(token_length):
    position = jnp.arange(token_length, dtype=jnp.int32)
    grid_row = (position // GRID).astype(jnp.float32)
    grid_col = (position % GRID).astype(jnp.float32)
    half_pairs = HEAD_CHANNELS // 4
    inv_freq = rope_base ** (-jnp.arange(half_pairs, dtype=jnp.float32) / half_pairs)
    angles = jnp.concatenate([grid_row[:, None] * inv_freq, grid_col[:, None] * inv_freq], axis=1)
    return (jnp.cos(angles), jnp.sin(angles))


def rotate(vector, cos_tab, sin_tab):
    even_part = vector[..., 0::2]
    odd_part = vector[..., 1::2]
    turned = jnp.stack(
        [even_part * cos_tab - odd_part * sin_tab, even_part * sin_tab + odd_part * cos_tab],
        axis=-1,
    )
    return turned.reshape(vector.shape)


def rotate_back(cotangent, cos_tab, sin_tab):
    even_part = cotangent[..., 0::2]
    odd_part = cotangent[..., 1::2]
    turned = jnp.stack(
        [even_part * cos_tab + odd_part * sin_tab, odd_part * cos_tab - even_part * sin_tab],
        axis=-1,
    )
    return turned.reshape(cotangent.shape)


def inverse_rms(vector):
    return lax.rsqrt(jnp.mean(vector * vector, axis=-1, keepdims=True) + norm_eps)


def norm_back(vector, inv_scale, cotangent, gain_vec):
    weighted = cotangent * gain_vec
    inner_mean = jnp.mean(weighted * vector, axis=-1, keepdims=True)
    return inv_scale * (weighted - vector * inv_scale * inv_scale * inner_mean)


def head_grads(
    query_in, key_input, value_input, grad_in, query_gain, key_gain, cos_tab, sin_tab, block_rows
):
    token_length, groups, per_group, head_dim = query_in.shape
    cos_four = cos_tab[:, None, None, :]
    sin_four = sin_tab[:, None, None, :]
    cos_three = cos_tab[:, None, :]
    sin_three = sin_tab[:, None, :]
    query_f = query_in.astype(jnp.float32)
    query_inv = inverse_rms(query_f)
    query_rot = rotate(query_f * query_inv * query_gain, cos_four, sin_four).astype(jnp.bfloat16)
    key_f = key_input.astype(jnp.float32)
    key_inv = inverse_rms(key_f)
    key_rot = rotate(key_f * key_inv * key_gain, cos_three, sin_three).astype(jnp.bfloat16)
    num_blocks = token_length // block_rows
    query_blocks = query_rot.reshape(num_blocks, block_rows, groups, per_group, head_dim)
    grad_blocks = grad_in.reshape(num_blocks, block_rows, groups, per_group, head_dim)

    def attend_block(carried, pieces):
        key_acc, value_acc = carried
        query_piece, grad_piece = pieces
        scores = product("qgrd,cgd->grqc", query_piece, key_rot) * score_scale
        row_max = jnp.max(scores, axis=-1, keepdims=True)
        shifted = jnp.exp(scores - row_max)
        attn_prob = shifted / jnp.sum(shifted, axis=-1, keepdims=True)
        prob_low = attn_prob.astype(jnp.bfloat16)
        prob_grad = product("qgrd,cgd->grqc", grad_piece, value_input)
        row_dot = jnp.sum(attn_prob * prob_grad, axis=-1, keepdims=True)
        score_grad = (attn_prob * (prob_grad - row_dot) * score_scale).astype(jnp.bfloat16)
        dq_piece = product("grqc,cgd->qgrd", score_grad, key_rot)
        key_acc = key_acc + product("grqc,qgrd->cgd", score_grad, query_piece)
        value_acc = value_acc + product("grqc,qgrd->cgd", prob_low, grad_piece)
        return ((key_acc, value_acc), dq_piece)

    empty_acc = jnp.zeros((token_length, groups, head_dim), jnp.float32)
    (key_rot_grad, value_acc), query_rot_grad = lax.scan(
        attend_block, (empty_acc, empty_acc), (query_blocks, grad_blocks)
    )
    query_rot_grad = query_rot_grad.reshape(token_length, groups, per_group, head_dim)
    query_grad = norm_back(
        query_f, query_inv, rotate_back(query_rot_grad, cos_four, sin_four), query_gain
    ).astype(jnp.bfloat16)
    key_portion = norm_back(
        key_f, key_inv, rotate_back(key_rot_grad, cos_three, sin_three), key_gain
    ).astype(jnp.bfloat16)
    return (query_grad, key_portion, value_acc.astype(jnp.bfloat16))


def on_device(
    inputs, queries, keys, values, out_grad, query_gain, key_gain, key_matrix, value_matrix
):
    sp_count = lax.axis_size("sp")
    dp_count = lax.axis_size("dp")
    token_row_block = inputs.shape[1]
    token_length = token_row_block * sp_count
    local_heads = QUERY_HEADS // sp_count
    portion_heads = min(local_heads, QUERY_HEADS // KEY_VALUE_HEADS)
    kv_here = local_heads // portion_heads
    group_copies = QUERY_HEADS // KEY_VALUE_HEADS // portion_heads
    key_value_width = KEY_VALUE_HEADS * HEAD_CHANNELS
    key_positions = jnp.repeat(
        keys[0].reshape(token_row_block, KEY_VALUE_HEADS, HEAD_CHANNELS), group_copies, axis=1
    ).reshape(token_row_block, key_value_width * group_copies)
    value_positions = jnp.repeat(
        values[0].reshape(token_row_block, KEY_VALUE_HEADS, HEAD_CHANNELS), group_copies, axis=1
    ).reshape(token_row_block, key_value_width * group_copies)
    grad_heads, query_heads, key_heads, value_heads = (
        lax.all_to_all(out_grad[0], "sp", split_axis=1, concat_axis=0, tiled=True),
        lax.all_to_all(queries[0], "sp", split_axis=1, concat_axis=0, tiled=True),
        lax.all_to_all(key_positions, "sp", split_axis=1, concat_axis=0, tiled=True),
        lax.all_to_all(value_positions, "sp", split_axis=1, concat_axis=0, tiled=True),
    )
    cos_tab, sin_tab = rotary_tables(token_length)
    query_part, key_portion, value_portion = head_grads(
        query_heads.reshape(token_length, kv_here, portion_heads, HEAD_CHANNELS),
        key_heads.reshape(token_length, kv_here, HEAD_CHANNELS),
        value_heads.reshape(token_length, kv_here, HEAD_CHANNELS),
        grad_heads.reshape(token_length, kv_here, portion_heads, HEAD_CHANNELS),
        query_gain,
        key_gain,
        cos_tab,
        sin_tab,
        min(512, token_length),
    )
    query_tokens, key_token_rows, value_token_rows = (
        lax.all_to_all(
            query_part.reshape(token_length, local_heads * HEAD_CHANNELS),
            "sp",
            split_axis=0,
            concat_axis=1,
            tiled=True,
        ),
        lax.all_to_all(
            key_portion.reshape(token_length, kv_here * HEAD_CHANNELS),
            "sp",
            split_axis=0,
            concat_axis=1,
            tiled=True,
        ),
        lax.all_to_all(
            value_portion.reshape(token_length, kv_here * HEAD_CHANNELS),
            "sp",
            split_axis=0,
            concat_axis=1,
            tiled=True,
        ),
    )
    key_gradient = (
        key_token_rows.reshape(token_row_block, KEY_VALUE_HEADS, group_copies, HEAD_CHANNELS)
        .astype(jnp.float32)
        .sum(axis=2)
        .astype(jnp.bfloat16)
    )
    value_gradient = (
        value_token_rows.reshape(token_row_block, KEY_VALUE_HEADS, group_copies, HEAD_CHANNELS)
        .astype(jnp.float32)
        .sum(axis=2)
        .astype(jnp.bfloat16)
    )
    projection_gradient = jnp.concatenate(
        [
            key_gradient.reshape(token_row_block, key_value_width),
            value_gradient.reshape(token_row_block, key_value_width),
        ],
        axis=1,
    )
    joined_weight = jnp.concatenate([key_matrix, value_matrix], axis=1)
    input_grad = lax.dot_general(
        projection_gradient,
        lax.all_gather(joined_weight, "dp", axis=0, tiled=True),
        (((1,), (1,)), ((), ())),
        preferred_element_type=jnp.float32,
    ).astype(jnp.bfloat16)
    token_in = inputs[0]
    width = inputs.shape[2]
    row_share = width // (sp_count * dp_count)
    permuted = (
        token_in.reshape(token_row_block, dp_count, sp_count, row_share)
        .transpose(0, 2, 1, 3)
        .reshape(token_row_block, width)
    )
    share_cols = lax.all_to_all(permuted, "sp", split_axis=1, concat_axis=0, tiled=True)
    all_grads = lax.all_gather(projection_gradient, "sp", axis=0, tiled=True)
    grad_piece = lax.psum_scatter(
        lax.dot_general(
            share_cols, all_grads, (((0,), (0,)), ((), ())), preferred_element_type=jnp.float32
        ).astype(jnp.bfloat16),
        "dp",
        scatter_dimension=0,
        tiled=True,
    ).astype(jnp.float32)
    weight_grad = lax.all_gather(grad_piece, "sp", axis=0, tiled=True)
    return (
        input_grad[None],
        query_tokens[None],
        weight_grad[:, :key_value_width],
        weight_grad[:, key_value_width:],
    )


LANES = 128
MESH = pl.DeviceIdType.MESH
F32 = jnp.float32
BF16 = jnp.bfloat16


def pair_tables(token_length):
    position = np.arange(token_length)
    half_pairs = HEAD_CHANNELS // 4
    inv_freq = (rope_base ** (-np.arange(half_pairs) / half_pairs)).astype(np.float32)
    row = (position // GRID).astype(np.float32)
    col = (position % GRID).astype(np.float32)
    angles = np.concatenate([row[:, None] * inv_freq, col[:, None] * inv_freq], axis=1)
    cos_tab = np.repeat(np.cos(angles), 2, axis=1)
    sin_tab = np.repeat(np.sin(angles), 2, axis=1)
    sin_tab[:, 0::2] *= -1.0
    return (
        np.tile(cos_tab, (1, 2)).astype(np.float32),
        np.tile(sin_tab, (1, 2)).astype(np.float32),
    )


def swap_pairs(x):
    lane = lax.broadcasted_iota(jnp.int32, x.shape, 1)
    return jnp.where(lane % 2 == 0, pltpu.roll(x, LANES - 1, 1), pltpu.roll(x, 1, 1))


def head_mean(z):
    row = lax.broadcasted_iota(jnp.int32, (LANES, LANES), 0) // HEAD_CHANNELS
    col = lax.broadcasted_iota(jnp.int32, (LANES, LANES), 1) // HEAD_CHANNELS
    ones = jnp.where(row == col, 1.0, 0.0).astype(BF16)
    high = z.astype(BF16)
    low = (z - high.astype(F32)).astype(BF16)
    total = jnp.dot(high, ones, preferred_element_type=F32)
    total = total + jnp.dot(low, ones, preferred_element_type=F32)
    return total * (1.0 / HEAD_CHANNELS)


def norm_rotate(x, gain, cos_tab, sin_tab):
    inv = lax.rsqrt(head_mean(x * x) + norm_eps)
    y = x * inv * gain
    return y * cos_tab + swap_pairs(y) * sin_tab


def norm_rotate_back(x, cotangent, gain, cos_tab, sin_tab):
    turned = cotangent * cos_tab - swap_pairs(cotangent) * sin_tab
    inv = lax.rsqrt(head_mean(x * x) + norm_eps)
    weighted = turned * gain
    return inv * (weighted - x * (inv * inv * head_mean(weighted * x)))


def contract(a, b, dims):
    return lax.dot_general(a, b, (dims, ((), ())), preferred_element_type=F32)


def step_kernel(
    n, dp,
    x_hbm, q_hbm, k_hbm, v_hbm, do_hbm, qg_ref, kg_ref, km_hbm, vm_hbm, cos_hbm, sin_hbm,
    dx_ref, dq_ref, kw_ref, vw_ref,
    q_buf, do_buf, cos_buf, sin_buf, k_all, v_all, x_all, wk_all, wv_all,
    q_st, do_st, k_st, v_st, dq_acc, part, got, g_all, x_t, wg_part, wg_got, fin_all,
    local_sem, kv_send, kv_recv, x_send, x_recv, w_send, w_recv, w_fsend,
    p_send, p_recv, g_send, g_recv, g_fsend, r_send, r_recv, f_send, f_recv,
):
    me = lax.axis_index("sp")
    md = lax.axis_index("dp")
    rows, q_width = q_buf.shape
    kv_width = k_all.shape[2]
    share = x_all.shape[2]
    kv_heads = kv_width // HEAD_CHANNELS
    per_group = q_width // kv_width
    mate = md + 1 - 2 * (md % 2)
    pairs = dp // 2

    def sp_peer(o):
        return lax.rem(me + o, n)

    def sp_from(o):
        return lax.rem(me - o + n, n)

    def dp_peer(o):
        return lax.rem(md + o, dp)

    def dp_from(o):
        return lax.rem(md - o + dp, dp)

    barrier = pltpu.get_barrier_semaphore()
    for o in range(1, n):
        pl.semaphore_signal(barrier, inc=1, device_id={"sp": sp_peer(o)}, device_id_type=MESH)
    for o in range(1, dp):
        pl.semaphore_signal(barrier, inc=1, device_id={"dp": dp_peer(o)}, device_id_type=MESH)

    def columns(d):
        return pl.ds(pl.multiple_of(d * share, share), share)

    local = [
        pltpu.make_async_copy(src, dst, local_sem.at[i])
        for i, (src, dst) in enumerate([
            (q_hbm, q_buf), (do_hbm, do_buf), (cos_hbm, cos_buf), (sin_hbm, sin_buf),
            (k_hbm, k_all.at[me]), (v_hbm, v_all.at[me]),
            (x_hbm.at[:, columns(md)], x_all.at[md]),
            (km_hbm, wk_all.at[md]), (vm_hbm, wv_all.at[md]),
        ])
    ]
    for copy in local:
        copy.start()

    def remote(src, dst, send, recv, where):
        return pltpu.make_async_remote_copy(
            src_ref=src, dst_ref=dst, send_sem=send, recv_sem=recv,
            device_id=where, device_id_type=MESH,
        )

    pl.semaphore_wait(barrier, n + dp - 2)

    sends = []

    def send(*args):
        copy = remote(*args)
        copy.start()
        sends.append(copy)

    def arrived(dst, recv):
        remote(dst, dst, recv, recv, {"sp": me}).wait_recv()

    order = sorted(range(1, n), key=lambda o: -min(o, n - o))
    for kind, (src, dst) in enumerate([(k_hbm, k_all), (v_hbm, v_all)]):
        for o in order:
            send(src, dst.at[me], kv_send.at[kind, o], kv_recv.at[kind, me], {"sp": sp_peer(o)})
    weights = [(km_hbm, wk_all), (vm_hbm, wv_all)]
    for kind, (src, dst) in enumerate(weights):
        for o in range(2, dp, 2):
            send(src, dst.at[md], w_send.at[kind, o], w_recv.at[kind, md], {"dp": dp_peer(o)})
        send(src, dst.at[md], w_send.at[kind, 1], w_recv.at[kind, md], {"dp": mate})
    for o in range(1, dp):
        send(x_hbm.at[:, columns(dp_peer(o))], x_all.at[md], x_send.at[o], x_recv.at[md],
             {"dp": dp_peer(o)})

    for copy in local:
        copy.wait()

    my_rows = pl.ds(pl.multiple_of(me * rows, rows), rows)
    cos_own = cos_buf[my_rows, :]
    sin_own = sin_buf[my_rows, :]
    q_gain = qg_ref[...]
    k_gain = kg_ref[...]

    for c in range(q_width // LANES):
        lanes = pl.ds(c * LANES, LANES)
        turned = norm_rotate(q_buf[:, lanes].astype(F32), q_gain, cos_own, sin_own).astype(BF16)
        grads = do_buf[:, lanes]
        for a in range(2):
            h = 2 * c + a
            to = pl.ds((h % per_group) * rows, rows)
            half = slice(a * HEAD_CHANNELS, (a + 1) * HEAD_CHANNELS)
            q_st[h // per_group, to, :] = turned[:, half]
            do_st[h // per_group, to, :] = grads[:, half]

    def stack_keys(src):
        at = pl.ds(pl.multiple_of(src * rows, rows), rows)
        for c in range(kv_width // LANES):
            lanes = pl.ds(c * LANES, LANES)
            turned = norm_rotate(
                k_all[src, :, lanes].astype(F32), k_gain, cos_buf[at, :], sin_buf[at, :]
            ).astype(BF16)
            vals = v_all[src, :, lanes]
            for a in range(2):
                half = slice(a * HEAD_CHANNELS, (a + 1) * HEAD_CHANNELS)
                k_st[2 * c + a, at, :] = turned[:, half]
                v_st[2 * c + a, at, :] = vals[:, half]

    stack_keys(me)
    for o in range(1, n):
        src = sp_from(o)
        arrived(k_all.at[src], kv_recv.at[0, src])
        arrived(v_all.at[src], kv_recv.at[1, src])
        stack_keys(src)

    def attend(g):
        qs = q_st[g]
        dos = do_st[g]
        ks = k_st[g]
        vs = v_st[g]
        scores = contract(ks, qs, ((1,), (1,))) * score_scale
        shifted = jnp.exp(scores - jnp.max(scores, axis=0, keepdims=True))
        prob = shifted * (1.0 / jnp.sum(shifted, axis=0, keepdims=True))
        value_part = contract(prob.astype(BF16), dos, ((1,), (0,)))
        prob_grad = contract(vs, dos, ((1,), (1,)))
        row_dot = jnp.sum(prob * prob_grad, axis=0, keepdims=True)
        score_grad = (prob * (prob_grad - row_dot) * score_scale).astype(BF16)
        key_part = contract(score_grad, qs, ((1,), (0,)))
        dq_t = contract(ks, score_grad, ((0,), (0,)))
        for r in range(0, per_group, 2):
            both = jnp.concatenate(
                [dq_t[:, r * rows:(r + 1) * rows], dq_t[:, (r + 1) * rows:(r + 2) * rows]], axis=0
            )
            head = g * per_group + r
            dq_acc[:, head * HEAD_CHANNELS:head * HEAD_CHANNELS + LANES] = both.T
        return key_part, value_part

    for c in range(kv_heads // 2):
        key_low, value_low = attend(2 * c)
        key_high, value_high = attend(2 * c + 1)
        both = jnp.concatenate([key_low, key_high, value_low, value_high], axis=1).astype(BF16)
        for j in range(n):
            part[c, j] = both[j * rows:(j + 1) * rows, :]
        for o in order:
            send(part.at[c, sp_peer(o)], got.at[c, me], p_send.at[c, o], p_recv.at[c, me],
                 {"sp": sp_peer(o)})

    for kind, (_, dst) in enumerate(weights):
        for o in range(2, dp, 2):
            src = dp_from(o)
            arrived(dst.at[src], w_recv.at[kind, src])
            send(dst.at[src], dst.at[src], w_fsend.at[kind, o], w_recv.at[kind, src], {"dp": mate})

    for c in range(q_width // LANES):
        lanes = pl.ds(c * LANES, LANES)
        dq_ref[:, lanes] = norm_rotate_back(
            q_buf[:, lanes].astype(F32), dq_acc[:, lanes], q_gain, cos_own, sin_own
        ).astype(BF16)

    for o in range(dp):
        src = dp_from(o)
        if o:
            arrived(x_all.at[src], x_recv.at[src])
        x_t[src] = x_all[src].T

    for c in range(kv_heads // 2):
        total = part[c, me].astype(F32)
        for o in range(1, n):
            src = sp_from(o)
            arrived(got.at[c, src], p_recv.at[c, src])
            total = total + got[c, src].astype(F32)
        lanes = pl.ds(c * LANES, LANES)
        g_all[md, :, lanes] = norm_rotate_back(
            k_all[me, :, lanes].astype(F32), total[:, :LANES], k_gain, cos_own, sin_own
        ).astype(BF16)
        g_all[md, :, pl.ds(kv_width + c * LANES, LANES)] = total[:, LANES:].astype(BF16)
    for o in range(2, dp, 2):
        send(g_all.at[md], g_all.at[md], g_send.at[o], g_recv.at[md], {"dp": dp_peer(o)})
    send(g_all.at[md], g_all.at[md], g_send.at[1], g_recv.at[md], {"dp": mate})

    own = g_all[md]
    wgrad = contract(x_t[md], own, ((1,), (0,)))

    def project(src):
        out = contract(own[:, :kv_width], wk_all[src], ((1,), (1,)))
        out = out + contract(own[:, kv_width:], wv_all[src], ((1,), (1,)))
        dx_ref[:, columns(src)] = out.astype(BF16)

    project(md)
    for o in range(2, dp, 2):
        project(dp_from(o))
    for o in range(2, dp, 2):
        src = dp_from(o)
        arrived(g_all.at[src], g_recv.at[src])
        send(g_all.at[src], g_all.at[src], g_fsend.at[o], g_recv.at[src], {"dp": mate})
        wgrad = wgrad + contract(x_t[src], g_all[src], ((1,), (0,)))
    for o in range(0, dp, 2):
        src = lax.rem(mate - o + dp, dp)
        arrived(g_all.at[src], g_recv.at[src])
        wgrad = wgrad + contract(x_t[src], g_all[src], ((1,), (0,)))

    piece = share // n
    for j in range(n):
        wg_part[j] = wgrad[j * piece:(j + 1) * piece, :].astype(BF16)
    for o in order:
        send(wg_part.at[sp_peer(o)], wg_got.at[me], r_send.at[o], r_recv.at[me],
             {"sp": sp_peer(o)})
    for o in range(0, dp, 2):
        src = lax.rem(mate - o + dp, dp)
        for kind, (_, dst) in enumerate(weights):
            arrived(dst.at[src], w_recv.at[kind, src])
        project(src)
    total = wg_part[me].astype(F32)
    for o in range(1, n):
        src = sp_from(o)
        arrived(wg_got.at[src], r_recv.at[src])
        total = total + wg_got[src].astype(F32)
    fin_all[me] = total.astype(BF16)
    for o in order:
        send(fin_all.at[me], fin_all.at[me], f_send.at[o], f_recv.at[me], {"sp": sp_peer(o)})
    for o in range(n):
        src = sp_from(o)
        if o:
            arrived(fin_all.at[src], f_recv.at[src])
        at = pl.ds(pl.multiple_of(src * piece, piece), piece)
        kw_ref[at, :] = fin_all[src, :, :kv_width].astype(F32)
        vw_ref[at, :] = fin_all[src, :, kv_width:].astype(F32)
    for copy in sends:
        copy.wait_send()


def kernel_step(
    n, dp, inputs, queries, keys, values, out_grad, query_gain, key_gain, key_matrix, value_matrix
):
    rows, width = inputs.shape[1:]
    q_width = queries.shape[2]
    kv_width = keys.shape[2]
    length = rows * n
    share = width // dp
    kv_heads = kv_width // HEAD_CHANNELS
    stack = rows * (q_width // kv_width)
    cos_tab, sin_tab = pair_tables(length)
    vmem = functools.partial(pltpu.VMEM)
    dma = pltpu.SemaphoreType.DMA
    scratch = [
        vmem((rows, q_width), BF16), vmem((rows, q_width), BF16),
        vmem((length, LANES), F32), vmem((length, LANES), F32),
        vmem((n, rows, kv_width), BF16), vmem((n, rows, kv_width), BF16),
        vmem((dp, rows, share), BF16),
        vmem((dp, share, kv_width), BF16), vmem((dp, share, kv_width), BF16),
        vmem((kv_heads, stack, HEAD_CHANNELS), BF16), vmem((kv_heads, stack, HEAD_CHANNELS), BF16),
        vmem((kv_heads, length, HEAD_CHANNELS), BF16), vmem((kv_heads, length, HEAD_CHANNELS), BF16),
        vmem((rows, q_width), F32),
        vmem((kv_heads // 2, n, rows, 2 * LANES), BF16),
        vmem((kv_heads // 2, n, rows, 2 * LANES), BF16),
        vmem((dp, rows, 2 * kv_width), BF16), vmem((dp, share, rows), BF16),
        vmem((n, share // n, 2 * kv_width), BF16), vmem((n, share // n, 2 * kv_width), BF16),
        vmem((n, share // n, 2 * kv_width), BF16),
        dma((9,)), dma((2, n)), dma((2, n)), dma((dp,)), dma((dp,)),
        dma((2, dp)), dma((2, dp)), dma((2, dp)),
        dma((kv_heads // 2, n)), dma((kv_heads // 2, n)),
        dma((dp,)), dma((dp,)), dma((dp,)), dma((n,)), dma((n,)), dma((n,)), dma((n,)),
    ]
    hbm = pl.BlockSpec(memory_space=pl.ANY)
    here = pl.BlockSpec(memory_space=pltpu.VMEM)
    dx, dq, kw, vw = pl.pallas_call(
        functools.partial(step_kernel, n, dp),
        out_shape=(
            jax.ShapeDtypeStruct((rows, width), BF16),
            jax.ShapeDtypeStruct((rows, q_width), BF16),
            jax.ShapeDtypeStruct((share, kv_width), F32),
            jax.ShapeDtypeStruct((share, kv_width), F32),
        ),
        in_specs=[hbm] * 5 + [here] * 2 + [hbm] * 4,
        out_specs=[here] * 4,
        scratch_shapes=scratch,
        compiler_params=pltpu.CompilerParams(
            collective_id=0, has_side_effects=True, vmem_limit_bytes=56 * 1024 * 1024
        ),
    )(
        inputs[0], queries[0], keys[0], values[0], out_grad[0],
        jnp.tile(query_gain, 2)[None], jnp.tile(key_gain, 2)[None],
        key_matrix, value_matrix, jnp.asarray(cos_tab), jnp.asarray(sin_tab),
    )
    return dx[None], dq[None], kw, vw


def device_step(inputs, *rest):
    n = lax.axis_size("sp")
    dp = lax.axis_size("dp")
    rows, width = inputs.shape[1:]
    fits = dp % 2 == 0 and width % (dp * LANES) == 0 and rows % LANES == 0 and rows * n <= 1024
    if fits and (width // dp) % (16 * n) == 0:
        return kernel_step(n, dp, inputs, *rest)
    return on_device(inputs, *rest)


def solution(mesh):
    return jax.shard_map(
        device_step,
        mesh=mesh,
        in_specs=(
            P("dp", "sp", None),
            P("dp", "sp", None),
            P("dp", "sp", None),
            P("dp", "sp", None),
            P("dp", "sp", None),
            P(),
            P(),
            P("dp", None),
            P("dp", None),
        ),
        out_specs=(P("dp", "sp", None), P("dp", "sp", None), P("dp", None), P("dp", None)),
        check_vma=False,
    )
```

```python
import functools

import jax
import jax.numpy as jnp
import numpy as np
from jax import lax
from jax.experimental import pallas as pl
from jax.experimental.pallas import tpu as pltpu
from jax.sharding import PartitionSpec as P

QUERY_HEADS = 16
KEY_VALUE_HEADS = 4
HEAD_CHANNELS = 64
GRID = 64


rope_base = 10000.0
norm_eps = 0.5
score_scale = 0.125


def product(pattern, first_op, second_op):
    return jnp.einsum(pattern, first_op, second_op, preferred_element_type=jnp.float32)


def rotary_tables(token_length):
    position = jnp.arange(token_length, dtype=jnp.int32)
    grid_row = (position // GRID).astype(jnp.float32)
    grid_col = (position % GRID).astype(jnp.float32)
    half_pairs = HEAD_CHANNELS // 4
    inv_freq = rope_base ** (-jnp.arange(half_pairs, dtype=jnp.float32) / half_pairs)
    angles = jnp.concatenate([grid_row[:, None] * inv_freq, grid_col[:, None] * inv_freq], axis=1)
    return (jnp.cos(angles), jnp.sin(angles))


def rotate(vector, cos_tab, sin_tab):
    even_part = vector[..., 0::2]
    odd_part = vector[..., 1::2]
    turned = jnp.stack(
        [even_part * cos_tab - odd_part * sin_tab, even_part * sin_tab + odd_part * cos_tab],
        axis=-1,
    )
    return turned.reshape(vector.shape)


def rotate_back(cotangent, cos_tab, sin_tab):
    even_part = cotangent[..., 0::2]
    odd_part = cotangent[..., 1::2]
    turned = jnp.stack(
        [even_part * cos_tab + odd_part * sin_tab, odd_part * cos_tab - even_part * sin_tab],
        axis=-1,
    )
    return turned.reshape(cotangent.shape)


def inverse_rms(vector):
    return lax.rsqrt(jnp.mean(vector * vector, axis=-1, keepdims=True) + norm_eps)


def norm_back(vector, inv_scale, cotangent, gain_vec):
    weighted = cotangent * gain_vec
    inner_mean = jnp.mean(weighted * vector, axis=-1, keepdims=True)
    return inv_scale * (weighted - vector * inv_scale * inv_scale * inner_mean)


def head_grads(
    query_in, key_input, value_input, grad_in, query_gain, key_gain, cos_tab, sin_tab, block_rows
):
    token_length, groups, per_group, head_dim = query_in.shape
    cos_four = cos_tab[:, None, None, :]
    sin_four = sin_tab[:, None, None, :]
    cos_three = cos_tab[:, None, :]
    sin_three = sin_tab[:, None, :]
    query_f = query_in.astype(jnp.float32)
    query_inv = inverse_rms(query_f)
    query_rot = rotate(query_f * query_inv * query_gain, cos_four, sin_four).astype(jnp.bfloat16)
    key_f = key_input.astype(jnp.float32)
    key_inv = inverse_rms(key_f)
    key_rot = rotate(key_f * key_inv * key_gain, cos_three, sin_three).astype(jnp.bfloat16)
    num_blocks = token_length // block_rows
    query_blocks = query_rot.reshape(num_blocks, block_rows, groups, per_group, head_dim)
    grad_blocks = grad_in.reshape(num_blocks, block_rows, groups, per_group, head_dim)

    def attend_block(carried, pieces):
        key_acc, value_acc = carried
        query_piece, grad_piece = pieces
        scores = product("qgrd,cgd->grqc", query_piece, key_rot) * score_scale
        row_max = jnp.max(scores, axis=-1, keepdims=True)
        shifted = jnp.exp(scores - row_max)
        attn_prob = shifted / jnp.sum(shifted, axis=-1, keepdims=True)
        prob_low = attn_prob.astype(jnp.bfloat16)
        prob_grad = product("qgrd,cgd->grqc", grad_piece, value_input)
        row_dot = jnp.sum(attn_prob * prob_grad, axis=-1, keepdims=True)
        score_grad = (attn_prob * (prob_grad - row_dot) * score_scale).astype(jnp.bfloat16)
        dq_piece = product("grqc,cgd->qgrd", score_grad, key_rot)
        key_acc = key_acc + product("grqc,qgrd->cgd", score_grad, query_piece)
        value_acc = value_acc + product("grqc,qgrd->cgd", prob_low, grad_piece)
        return ((key_acc, value_acc), dq_piece)

    empty_acc = jnp.zeros((token_length, groups, head_dim), jnp.float32)
    (key_rot_grad, value_acc), query_rot_grad = lax.scan(
        attend_block, (empty_acc, empty_acc), (query_blocks, grad_blocks)
    )
    query_rot_grad = query_rot_grad.reshape(token_length, groups, per_group, head_dim)
    query_grad = norm_back(
        query_f, query_inv, rotate_back(query_rot_grad, cos_four, sin_four), query_gain
    ).astype(jnp.bfloat16)
    key_portion = norm_back(
        key_f, key_inv, rotate_back(key_rot_grad, cos_three, sin_three), key_gain
    ).astype(jnp.bfloat16)
    return (query_grad, key_portion, value_acc.astype(jnp.bfloat16))


def on_device(
    inputs, queries, keys, values, out_grad, query_gain, key_gain, key_matrix, value_matrix
):
    sp_count = lax.axis_size("sp")
    dp_count = lax.axis_size("dp")
    token_row_block = inputs.shape[1]
    token_length = token_row_block * sp_count
    local_heads = QUERY_HEADS // sp_count
    portion_heads = min(local_heads, QUERY_HEADS // KEY_VALUE_HEADS)
    kv_here = local_heads // portion_heads
    group_copies = QUERY_HEADS // KEY_VALUE_HEADS // portion_heads
    key_value_width = KEY_VALUE_HEADS * HEAD_CHANNELS
    key_positions = jnp.repeat(
        keys[0].reshape(token_row_block, KEY_VALUE_HEADS, HEAD_CHANNELS), group_copies, axis=1
    ).reshape(token_row_block, key_value_width * group_copies)
    value_positions = jnp.repeat(
        values[0].reshape(token_row_block, KEY_VALUE_HEADS, HEAD_CHANNELS), group_copies, axis=1
    ).reshape(token_row_block, key_value_width * group_copies)
    grad_heads, query_heads, key_heads, value_heads = (
        lax.all_to_all(out_grad[0], "sp", split_axis=1, concat_axis=0, tiled=True),
        lax.all_to_all(queries[0], "sp", split_axis=1, concat_axis=0, tiled=True),
        lax.all_to_all(key_positions, "sp", split_axis=1, concat_axis=0, tiled=True),
        lax.all_to_all(value_positions, "sp", split_axis=1, concat_axis=0, tiled=True),
    )
    cos_tab, sin_tab = rotary_tables(token_length)
    query_part, key_portion, value_portion = head_grads(
        query_heads.reshape(token_length, kv_here, portion_heads, HEAD_CHANNELS),
        key_heads.reshape(token_length, kv_here, HEAD_CHANNELS),
        value_heads.reshape(token_length, kv_here, HEAD_CHANNELS),
        grad_heads.reshape(token_length, kv_here, portion_heads, HEAD_CHANNELS),
        query_gain,
        key_gain,
        cos_tab,
        sin_tab,
        min(512, token_length),
    )
    query_tokens, key_token_rows, value_token_rows = (
        lax.all_to_all(
            query_part.reshape(token_length, local_heads * HEAD_CHANNELS),
            "sp",
            split_axis=0,
            concat_axis=1,
            tiled=True,
        ),
        lax.all_to_all(
            key_portion.reshape(token_length, kv_here * HEAD_CHANNELS),
            "sp",
            split_axis=0,
            concat_axis=1,
            tiled=True,
        ),
        lax.all_to_all(
            value_portion.reshape(token_length, kv_here * HEAD_CHANNELS),
            "sp",
            split_axis=0,
            concat_axis=1,
            tiled=True,
        ),
    )
    key_gradient = (
        key_token_rows.reshape(token_row_block, KEY_VALUE_HEADS, group_copies, HEAD_CHANNELS)
        .astype(jnp.float32)
        .sum(axis=2)
        .astype(jnp.bfloat16)
    )
    value_gradient = (
        value_token_rows.reshape(token_row_block, KEY_VALUE_HEADS, group_copies, HEAD_CHANNELS)
        .astype(jnp.float32)
        .sum(axis=2)
        .astype(jnp.bfloat16)
    )
    projection_gradient = jnp.concatenate(
        [
            key_gradient.reshape(token_row_block, key_value_width),
            value_gradient.reshape(token_row_block, key_value_width),
        ],
        axis=1,
    )
    joined_weight = jnp.concatenate([key_matrix, value_matrix], axis=1)
    input_grad = lax.dot_general(
        projection_gradient,
        lax.all_gather(joined_weight, "dp", axis=0, tiled=True),
        (((1,), (1,)), ((), ())),
        preferred_element_type=jnp.float32,
    ).astype(jnp.bfloat16)
    token_in = inputs[0]
    width = inputs.shape[2]
    row_share = width // (sp_count * dp_count)
    permuted = (
        token_in.reshape(token_row_block, dp_count, sp_count, row_share)
        .transpose(0, 2, 1, 3)
        .reshape(token_row_block, width)
    )
    share_cols = lax.all_to_all(permuted, "sp", split_axis=1, concat_axis=0, tiled=True)
    all_grads = lax.all_gather(projection_gradient, "sp", axis=0, tiled=True)
    grad_piece = lax.psum_scatter(
        lax.dot_general(
            share_cols, all_grads, (((0,), (0,)), ((), ())), preferred_element_type=jnp.float32
        ).astype(jnp.bfloat16),
        "dp",
        scatter_dimension=0,
        tiled=True,
    ).astype(jnp.float32)
    weight_grad = lax.all_gather(grad_piece, "sp", axis=0, tiled=True)
    return (
        input_grad[None],
        query_tokens[None],
        weight_grad[:, :key_value_width],
        weight_grad[:, key_value_width:],
    )


LANES = 128
MESH = pl.DeviceIdType.MESH
F32 = jnp.float32
BF16 = jnp.bfloat16


def pair_tables(token_length):
    position = np.arange(token_length)
    half_pairs = HEAD_CHANNELS // 4
    inv_freq = (rope_base ** (-np.arange(half_pairs) / half_pairs)).astype(np.float32)
    row = (position // GRID).astype(np.float32)
    col = (position % GRID).astype(np.float32)
    angles = np.concatenate([row[:, None] * inv_freq, col[:, None] * inv_freq], axis=1)
    cos_tab = np.repeat(np.cos(angles), 2, axis=1)
    sin_tab = np.repeat(np.sin(angles), 2, axis=1)
    sin_tab[:, 0::2] *= -1.0
    return (
        np.tile(cos_tab, (1, 2)).astype(np.float32),
        np.tile(sin_tab, (1, 2)).astype(np.float32),
    )


def swap_pairs(x):
    lane = lax.broadcasted_iota(jnp.int32, x.shape, 1)
    return jnp.where(lane % 2 == 0, pltpu.roll(x, LANES - 1, 1), pltpu.roll(x, 1, 1))


def head_mean(z):
    row = lax.broadcasted_iota(jnp.int32, (LANES, LANES), 0) // HEAD_CHANNELS
    col = lax.broadcasted_iota(jnp.int32, (LANES, LANES), 1) // HEAD_CHANNELS
    ones = jnp.where(row == col, 1.0, 0.0).astype(BF16)
    high = z.astype(BF16)
    low = (z - high.astype(F32)).astype(BF16)
    total = jnp.dot(high, ones, preferred_element_type=F32)
    total = total + jnp.dot(low, ones, preferred_element_type=F32)
    return total * (1.0 / HEAD_CHANNELS)


def norm_rotate(x, gain, cos_tab, sin_tab):
    inv = lax.rsqrt(head_mean(x * x) + norm_eps)
    y = x * inv * gain
    return y * cos_tab + swap_pairs(y) * sin_tab


def norm_rotate_back(x, cotangent, gain, cos_tab, sin_tab):
    turned = cotangent * cos_tab - swap_pairs(cotangent) * sin_tab
    inv = lax.rsqrt(head_mean(x * x) + norm_eps)
    weighted = turned * gain
    return inv * (weighted - x * (inv * inv * head_mean(weighted * x)))


def contract(a, b, dims):
    return lax.dot_general(a, b, (dims, ((), ())), preferred_element_type=F32)


def step_kernel(
    n, dp,
    x_hbm, q_hbm, k_hbm, v_hbm, do_hbm, qg_ref, kg_ref, km_hbm, vm_hbm, cos_hbm, sin_hbm,
    dx_out, dq_out, fin_out,
    q_buf, do_buf, cos_buf, sin_buf, k_all, v_all, x_all, wk_all, wv_all,
    q_st, do_st, k_st, v_st, dq_acc, dq_buf, dx_buf, part, got, g_all, x_t, wg_part, wg_got,
    fin_all,
    local_sem, out_sem, kv_send, kv_recv, x_send, x_recv, w_send, w_recv, w_fsend,
    p_send, p_recv, g_send, g_recv, g_fsend, r_send, r_recv, f_send, f_recv,
):
    me = lax.axis_index("sp")
    md = lax.axis_index("dp")
    rows, q_width = q_buf.shape
    head_pairs = k_all.shape[0]
    share = x_all.shape[2]
    per_group = q_width // (2 * head_pairs * HEAD_CHANNELS)
    mate = md + 1 - 2 * (md % 2)
    piece = share // n

    def sp_peer(o):
        return lax.rem(me + o, n)

    def sp_from(o):
        return lax.rem(me - o + n, n)

    def dp_peer(o):
        return lax.rem(md + o, dp)

    def dp_from(o):
        return lax.rem(md - o + dp, dp)

    def mate_from(o):
        return lax.rem(mate - o + dp, dp)

    def pair(c):
        return pl.ds(c * LANES, LANES)

    barrier = pltpu.get_barrier_semaphore()
    for o in range(1, n):
        pl.semaphore_signal(barrier, inc=1, device_id={"sp": sp_peer(o)}, device_id_type=MESH)
    for o in range(1, dp):
        pl.semaphore_signal(barrier, inc=1, device_id={"dp": dp_peer(o)}, device_id_type=MESH)

    def columns(d):
        return pl.ds(pl.multiple_of(d * share, share), share)

    wanted = [
        (q_hbm, q_buf), (do_hbm, do_buf), (cos_hbm, cos_buf), (sin_hbm, sin_buf),
        (x_hbm.at[:, columns(md)], x_all.at[md]),
        (km_hbm, wk_all.at[md]), (vm_hbm, wv_all.at[md]),
    ]
    for c in range(head_pairs):
        wanted.append((k_hbm.at[:, pair(c)], k_all.at[c, me]))
        wanted.append((v_hbm.at[:, pair(c)], v_all.at[c, me]))
    local = [
        pltpu.make_async_copy(src, dst, local_sem.at[i]) for i, (src, dst) in enumerate(wanted)
    ]
    for copy in local:
        copy.start()

    def remote(src, dst, send, recv, where):
        return pltpu.make_async_remote_copy(
            src_ref=src, dst_ref=dst, send_sem=send, recv_sem=recv,
            device_id=where, device_id_type=MESH,
        )

    pl.semaphore_wait(barrier, n + dp - 2)

    sends = []

    def send(*args):
        copy = remote(*args)
        copy.start()
        sends.append(copy)

    def arrived(dst, recv):
        remote(dst, dst, recv, recv, {"sp": me}).wait_recv()

    order = sorted(range(1, n), key=lambda o: -min(o, n - o))
    for c in range(head_pairs):
        for kind, (src, dst) in enumerate([(k_hbm, k_all), (v_hbm, v_all)]):
            for o in order:
                send(src.at[:, pair(c)], dst.at[c, me], kv_send.at[kind, c, o],
                     kv_recv.at[kind, c, me], {"sp": sp_peer(o)})
    weights = [(km_hbm, wk_all), (vm_hbm, wv_all)]
    for kind, (src, dst) in enumerate(weights):
        for o in range(2, dp, 2):
            send(src, dst.at[md], w_send.at[kind, o], w_recv.at[kind, md], {"dp": dp_peer(o)})
        send(src, dst.at[md], w_send.at[kind, 1], w_recv.at[kind, md], {"dp": mate})
    for o in range(1, dp):
        send(x_hbm.at[:, columns(dp_peer(o))], x_all.at[md], x_send.at[o], x_recv.at[md],
             {"dp": dp_peer(o)})

    for copy in local:
        copy.wait()

    my_rows = pl.ds(pl.multiple_of(me * rows, rows), rows)
    cos_own = cos_buf[my_rows, :]
    sin_own = sin_buf[my_rows, :]
    q_gain = jnp.concatenate([qg_ref[...], qg_ref[...]], axis=1)
    k_gain = jnp.concatenate([kg_ref[...], kg_ref[...]], axis=1)

    for c in range(q_width // LANES):
        turned = norm_rotate(q_buf[:, pair(c)].astype(F32), q_gain, cos_own, sin_own).astype(BF16)
        grads = do_buf[:, pair(c)]
        for a in range(2):
            h = 2 * c + a
            to = pl.ds((h % per_group) * rows, rows)
            half = slice(a * HEAD_CHANNELS, (a + 1) * HEAD_CHANNELS)
            q_st[h // per_group, to, :] = turned[:, half]
            do_st[h // per_group, to, :] = grads[:, half]

    def stack_keys(c, src):
        at = pl.ds(pl.multiple_of(src * rows, rows), rows)
        turned = norm_rotate(
            k_all[c, src].astype(F32), k_gain, cos_buf[at, :], sin_buf[at, :]
        ).astype(BF16)
        vals = v_all[c, src]
        for a in range(2):
            half = slice(a * HEAD_CHANNELS, (a + 1) * HEAD_CHANNELS)
            k_st[2 * c + a, at, :] = turned[:, half]
            v_st[2 * c + a, at, :] = vals[:, half]

    def attend(g):
        qs = q_st[g]
        dos = do_st[g]
        ks = k_st[g]
        vs = v_st[g]
        scores = contract(ks, qs, ((1,), (1,))) * score_scale
        shifted = jnp.exp(scores - jnp.max(scores, axis=0, keepdims=True))
        prob = shifted * (1.0 / jnp.sum(shifted, axis=0, keepdims=True))
        value_part = contract(prob.astype(BF16), dos, ((1,), (0,)))
        prob_grad = contract(vs, dos, ((1,), (1,)))
        row_dot = jnp.sum(prob * prob_grad, axis=0, keepdims=True)
        score_grad = (prob * (prob_grad - row_dot) * score_scale).astype(BF16)
        key_part = contract(score_grad, qs, ((1,), (0,)))
        dq_t = contract(ks, score_grad, ((0,), (0,)))
        for r in range(0, per_group, 2):
            both = jnp.concatenate(
                [dq_t[:, r * rows:(r + 1) * rows], dq_t[:, (r + 1) * rows:(r + 2) * rows]], axis=0
            )
            head = g * per_group + r
            dq_acc[:, head * HEAD_CHANNELS:head * HEAD_CHANNELS + LANES] = both.T
        return key_part, value_part

    for c in range(head_pairs):
        stack_keys(c, me)
    for c in range(head_pairs):
        for o in range(1, n):
            src = sp_from(o)
            arrived(k_all.at[c, src], kv_recv.at[0, c, src])
            arrived(v_all.at[c, src], kv_recv.at[1, c, src])
            stack_keys(c, src)
        key_low, value_low = attend(2 * c)
        key_high, value_high = attend(2 * c + 1)
        both = jnp.concatenate([key_low, key_high, value_low, value_high], axis=1).astype(BF16)
        for j in range(n):
            part[c, j] = both[j * rows:(j + 1) * rows, :]
        for o in order:
            send(part.at[c, sp_peer(o)], got.at[c, me], p_send.at[c, o], p_recv.at[c, me],
                 {"sp": sp_peer(o)})

    def own_grads(c):
        total = part[c, me].astype(F32)
        for o in range(1, n):
            src = sp_from(o)
            arrived(got.at[c, src], p_recv.at[c, src])
            total = total + got[c, src].astype(F32)
        g_all[c, md, :, :LANES] = norm_rotate_back(
            k_all[c, me].astype(F32), total[:, :LANES], k_gain, cos_own, sin_own
        ).astype(BF16)
        g_all[c, md, :, LANES:] = total[:, LANES:].astype(BF16)
        mine = g_all.at[c, md]
        for o in range(2, dp, 2):
            send(mine, mine, g_send.at[c, o], g_recv.at[c, md], {"dp": dp_peer(o)})
        send(mine, mine, g_send.at[c, 1], g_recv.at[c, md], {"dp": mate})

    def pass_on(c):
        for o in range(2, dp, 2):
            src = dp_from(o)
            theirs = g_all.at[c, src]
            arrived(theirs, g_recv.at[c, src])
            send(theirs, theirs, g_fsend.at[c, o], g_recv.at[c, src], {"dp": mate})

    def weight_grads(c):
        total = contract(x_t[md], g_all[c, md], ((1,), (0,)))
        for o in range(2, dp, 2):
            src = dp_from(o)
            total = total + contract(x_t[src], g_all[c, src], ((1,), (0,)))
        for o in range(0, dp, 2):
            src = mate_from(o)
            arrived(g_all.at[c, src], g_recv.at[c, src])
            total = total + contract(x_t[src], g_all[c, src], ((1,), (0,)))
        for j in range(n):
            wg_part[c, j] = total[j * piece:(j + 1) * piece, :].astype(BF16)
        for o in order:
            send(wg_part.at[c, sp_peer(o)], wg_got.at[c, me], r_send.at[c, o], r_recv.at[c, me],
                 {"sp": sp_peer(o)})

    def sum_weight_grads(c):
        total = wg_part[c, me].astype(F32)
        for o in range(1, n):
            src = sp_from(o)
            arrived(wg_got.at[c, src], r_recv.at[c, src])
            total = total + wg_got[c, src].astype(F32)
        fin_all[c, me] = total.astype(BF16)
        mine = fin_all.at[c, me]
        for o in order:
            send(mine, mine, f_send.at[c, o], f_recv.at[c, me], {"sp": sp_peer(o)})

    for o in range(dp):
        src = dp_from(o)
        if o:
            arrived(x_all.at[src], x_recv.at[src])
        x_t[src] = x_all[src].T

    for c in range(head_pairs):
        own_grads(c)
        if c == 0:
            for kind, (_, dst) in enumerate(weights):
                for o in range(2, dp, 2):
                    src = dp_from(o)
                    arrived(dst.at[src], w_recv.at[kind, src])
                    send(dst.at[src], dst.at[src], w_fsend.at[kind, o], w_recv.at[kind, src],
                         {"dp": mate})
            for i in range(q_width // LANES):
                dq_buf[:, pair(i)] = norm_rotate_back(
                    q_buf[:, pair(i)].astype(F32), dq_acc[:, pair(i)], q_gain, cos_own, sin_own
                ).astype(BF16)
            dq_copy = pltpu.make_async_copy(dq_buf, dq_out, out_sem.at[0])
            dq_copy.start()

    own = jnp.concatenate(
        [g_all[c, md, :, :LANES] for c in range(head_pairs)]
        + [g_all[c, md, :, LANES:] for c in range(head_pairs)], axis=1)
    kv_width = head_pairs * LANES

    def project(src):
        out = contract(own[:, :kv_width], wk_all[src], ((1,), (1,)))
        out = out + contract(own[:, kv_width:], wv_all[src], ((1,), (1,)))
        dx_buf[:, columns(src)] = out.astype(BF16)

    for c in range(head_pairs):
        pass_on(c)
        weight_grads(c)
    for o in range(0, dp, 2):
        project(dp_from(o))
    for o in range(0, dp, 2):
        src = mate_from(o)
        for kind, (_, dst) in enumerate(weights):
            arrived(dst.at[src], w_recv.at[kind, src])
        project(src)
    dx_copy = pltpu.make_async_copy(dx_buf, dx_out, out_sem.at[1])
    dx_copy.start()
    for c in range(head_pairs):
        sum_weight_grads(c)
    for c in range(head_pairs):
        for o in range(1, n):
            src = sp_from(o)
            arrived(fin_all.at[c, src], f_recv.at[c, src])
    fin_copy = pltpu.make_async_copy(fin_all, fin_out, out_sem.at[2])
    fin_copy.start()
    for copy in sends:
        copy.wait_send()
    dq_copy.wait()
    dx_copy.wait()
    fin_copy.wait()


def write_kernel(dx_hbm, dq_hbm, fin_hbm, dx_out, dq_out, kw_out, vw_out,
                 dx_buf, dq_buf, fin_buf, kw_buf, vw_buf, in_sem, out_sem):
    loads = [
        pltpu.make_async_copy(src, dst, in_sem.at[i])
        for i, (src, dst) in enumerate([(fin_hbm, fin_buf), (dx_hbm, dx_buf), (dq_hbm, dq_buf)])
    ]
    stores = [
        pltpu.make_async_copy(src, dst, out_sem.at[i])
        for i, (src, dst) in enumerate(
            [(dx_buf, dx_out), (dq_buf, dq_out), (kw_buf, kw_out), (vw_buf, vw_out)])
    ]
    for copy in loads:
        copy.start()
    head_pairs, n, piece, _ = fin_buf.shape
    loads[0].wait()
    for c in range(head_pairs):
        for j in range(n):
            at = pl.ds(j * piece, piece)
            kw_buf[at, pl.ds(c * LANES, LANES)] = fin_buf[c, j, :, :LANES].astype(F32)
            vw_buf[at, pl.ds(c * LANES, LANES)] = fin_buf[c, j, :, LANES:].astype(F32)
    stores[2].start()
    stores[3].start()
    loads[1].wait()
    stores[0].start()
    loads[2].wait()
    stores[1].start()
    for copy in stores:
        copy.wait()


def kernel_step(
    n, dp, inputs, queries, keys, values, out_grad, query_gain, key_gain, key_matrix, value_matrix
):
    rows, width = inputs.shape[1:]
    q_width = queries.shape[2]
    kv_width = keys.shape[2]
    length = rows * n
    share = width // dp
    kv_heads = kv_width // HEAD_CHANNELS
    half = kv_heads // 2
    stack = rows * (q_width // kv_width)
    cos_tab, sin_tab = pair_tables(length)
    vmem = pltpu.VMEM
    dma = pltpu.SemaphoreType.DMA
    wide = 2 * LANES
    scratch = [
        vmem((rows, q_width), BF16), vmem((rows, q_width), BF16),
        vmem((length, LANES), F32), vmem((length, LANES), F32),
        vmem((half, n, rows, LANES), BF16), vmem((half, n, rows, LANES), BF16),
        vmem((dp, rows, share), BF16),
        vmem((dp, share, kv_width), BF16), vmem((dp, share, kv_width), BF16),
        vmem((kv_heads, stack, HEAD_CHANNELS), BF16), vmem((kv_heads, stack, HEAD_CHANNELS), BF16),
        vmem((kv_heads, length, HEAD_CHANNELS), BF16), vmem((kv_heads, length, HEAD_CHANNELS), BF16),
        vmem((rows, q_width), F32), vmem((rows, q_width), BF16), vmem((rows, width), BF16),
        vmem((half, n, rows, wide), BF16), vmem((half, n, rows, wide), BF16),
        vmem((half, dp, rows, wide), BF16), vmem((dp, share, rows), BF16),
        vmem((half, n, share // n, wide), BF16), vmem((half, n, share // n, wide), BF16),
        vmem((half, n, share // n, wide), BF16),
        dma((7 + 2 * half,)), dma((3,)),
        dma((2, half, n)), dma((2, half, n)), dma((dp,)), dma((dp,)),
        dma((2, dp)), dma((2, dp)), dma((2, dp)),
        dma((half, n)), dma((half, n)),
        dma((half, dp)), dma((half, dp)), dma((half, dp)),
        dma((half, n)), dma((half, n)), dma((half, n)), dma((half, n)),
    ]
    hbm = pl.BlockSpec(memory_space=pl.ANY)
    here = pl.BlockSpec(memory_space=pltpu.VMEM)
    dx_type = jax.ShapeDtypeStruct((rows, width), BF16)
    dq_type = jax.ShapeDtypeStruct((rows, q_width), BF16)
    kw_type = jax.ShapeDtypeStruct((share, kv_width), F32)
    fin_shape = (half, n, share // n, wide)
    dx, dq, fin = pl.pallas_call(
        functools.partial(step_kernel, n, dp),
        out_shape=(dx_type, dq_type, jax.ShapeDtypeStruct(fin_shape, BF16)),
        in_specs=[hbm] * 5 + [here] * 2 + [hbm] * 4,
        out_specs=[hbm] * 3,
        scratch_shapes=scratch,
        compiler_params=pltpu.CompilerParams(
            collective_id=0, has_side_effects=True, vmem_limit_bytes=56 * 1024 * 1024
        ),
    )(
        inputs[0], queries[0], keys[0], values[0], out_grad[0],
        query_gain[None], key_gain[None],
        key_matrix, value_matrix, jnp.asarray(cos_tab), jnp.asarray(sin_tab),
    )
    dx, dq, kw, vw = pl.pallas_call(
        write_kernel,
        out_shape=(dx_type, dq_type, kw_type, kw_type),
        in_specs=[hbm] * 3,
        out_specs=[hbm] * 4,
        scratch_shapes=[
            vmem((rows, width), BF16), vmem((rows, q_width), BF16), vmem(fin_shape, BF16),
            vmem((share, kv_width), F32), vmem((share, kv_width), F32), dma((3,)), dma((4,)),
        ],
    )(dx, dq, fin)
    return dx[None], dq[None], kw, vw


def device_step(inputs, *rest):
    n = lax.axis_size("sp")
    dp = lax.axis_size("dp")
    rows, width = inputs.shape[1:]
    fits = dp % 2 == 0 and width % (dp * LANES) == 0 and rows % LANES == 0 and rows * n <= 1024
    if fits and (width // dp) % (16 * n) == 0:
        return kernel_step(n, dp, inputs, *rest)
    return on_device(inputs, *rest)


def solution(mesh):
    return jax.shard_map(
        device_step,
        mesh=mesh,
        in_specs=(
            P("dp", "sp", None),
            P("dp", "sp", None),
            P("dp", "sp", None),
            P("dp", "sp", None),
            P("dp", "sp", None),
            P(),
            P(),
            P("dp", None),
            P("dp", None),
        ),
        out_specs=(P("dp", "sp", None), P("dp", "sp", None), P("dp", None), P("dp", None)),
        check_vma=False,
    )
```

```python
import functools

import jax
import jax.numpy as jnp
import numpy as np
from jax import lax
from jax.experimental import pallas as pl
from jax.experimental.pallas import tpu as pltpu
from jax.sharding import PartitionSpec as P

QUERY_HEADS = 16
KEY_VALUE_HEADS = 4
HEAD_CHANNELS = 64
GRID = 64


rope_base = 10000.0
norm_eps = 0.5
score_scale = 0.125


def product(pattern, first_op, second_op):
    return jnp.einsum(pattern, first_op, second_op, preferred_element_type=jnp.float32)


def rotary_tables(token_length):
    position = jnp.arange(token_length, dtype=jnp.int32)
    grid_row = (position // GRID).astype(jnp.float32)
    grid_col = (position % GRID).astype(jnp.float32)
    half_pairs = HEAD_CHANNELS // 4
    inv_freq = rope_base ** (-jnp.arange(half_pairs, dtype=jnp.float32) / half_pairs)
    angles = jnp.concatenate([grid_row[:, None] * inv_freq, grid_col[:, None] * inv_freq], axis=1)
    return (jnp.cos(angles), jnp.sin(angles))


def rotate(vector, cos_tab, sin_tab):
    even_part = vector[..., 0::2]
    odd_part = vector[..., 1::2]
    turned = jnp.stack(
        [even_part * cos_tab - odd_part * sin_tab, even_part * sin_tab + odd_part * cos_tab],
        axis=-1,
    )
    return turned.reshape(vector.shape)


def rotate_back(cotangent, cos_tab, sin_tab):
    even_part = cotangent[..., 0::2]
    odd_part = cotangent[..., 1::2]
    turned = jnp.stack(
        [even_part * cos_tab + odd_part * sin_tab, odd_part * cos_tab - even_part * sin_tab],
        axis=-1,
    )
    return turned.reshape(cotangent.shape)


def inverse_rms(vector):
    return lax.rsqrt(jnp.mean(vector * vector, axis=-1, keepdims=True) + norm_eps)


def norm_back(vector, inv_scale, cotangent, gain_vec):
    weighted = cotangent * gain_vec
    inner_mean = jnp.mean(weighted * vector, axis=-1, keepdims=True)
    return inv_scale * (weighted - vector * inv_scale * inv_scale * inner_mean)


def head_grads(
    query_in, key_input, value_input, grad_in, query_gain, key_gain, cos_tab, sin_tab, block_rows
):
    token_length, groups, per_group, head_dim = query_in.shape
    cos_four = cos_tab[:, None, None, :]
    sin_four = sin_tab[:, None, None, :]
    cos_three = cos_tab[:, None, :]
    sin_three = sin_tab[:, None, :]
    query_f = query_in.astype(jnp.float32)
    query_inv = inverse_rms(query_f)
    query_rot = rotate(query_f * query_inv * query_gain, cos_four, sin_four).astype(jnp.bfloat16)
    key_f = key_input.astype(jnp.float32)
    key_inv = inverse_rms(key_f)
    key_rot = rotate(key_f * key_inv * key_gain, cos_three, sin_three).astype(jnp.bfloat16)
    num_blocks = token_length // block_rows
    query_blocks = query_rot.reshape(num_blocks, block_rows, groups, per_group, head_dim)
    grad_blocks = grad_in.reshape(num_blocks, block_rows, groups, per_group, head_dim)

    def attend_block(carried, pieces):
        key_acc, value_acc = carried
        query_piece, grad_piece = pieces
        scores = product("qgrd,cgd->grqc", query_piece, key_rot) * score_scale
        row_max = jnp.max(scores, axis=-1, keepdims=True)
        shifted = jnp.exp(scores - row_max)
        attn_prob = shifted / jnp.sum(shifted, axis=-1, keepdims=True)
        prob_low = attn_prob.astype(jnp.bfloat16)
        prob_grad = product("qgrd,cgd->grqc", grad_piece, value_input)
        row_dot = jnp.sum(attn_prob * prob_grad, axis=-1, keepdims=True)
        score_grad = (attn_prob * (prob_grad - row_dot) * score_scale).astype(jnp.bfloat16)
        dq_piece = product("grqc,cgd->qgrd", score_grad, key_rot)
        key_acc = key_acc + product("grqc,qgrd->cgd", score_grad, query_piece)
        value_acc = value_acc + product("grqc,qgrd->cgd", prob_low, grad_piece)
        return ((key_acc, value_acc), dq_piece)

    empty_acc = jnp.zeros((token_length, groups, head_dim), jnp.float32)
    (key_rot_grad, value_acc), query_rot_grad = lax.scan(
        attend_block, (empty_acc, empty_acc), (query_blocks, grad_blocks)
    )
    query_rot_grad = query_rot_grad.reshape(token_length, groups, per_group, head_dim)
    query_grad = norm_back(
        query_f, query_inv, rotate_back(query_rot_grad, cos_four, sin_four), query_gain
    ).astype(jnp.bfloat16)
    key_portion = norm_back(
        key_f, key_inv, rotate_back(key_rot_grad, cos_three, sin_three), key_gain
    ).astype(jnp.bfloat16)
    return (query_grad, key_portion, value_acc.astype(jnp.bfloat16))


def on_device(
    inputs, queries, keys, values, out_grad, query_gain, key_gain, key_matrix, value_matrix
):
    sp_count = lax.axis_size("sp")
    dp_count = lax.axis_size("dp")
    token_row_block = inputs.shape[1]
    token_length = token_row_block * sp_count
    local_heads = QUERY_HEADS // sp_count
    portion_heads = min(local_heads, QUERY_HEADS // KEY_VALUE_HEADS)
    kv_here = local_heads // portion_heads
    group_copies = QUERY_HEADS // KEY_VALUE_HEADS // portion_heads
    key_value_width = KEY_VALUE_HEADS * HEAD_CHANNELS
    key_positions = jnp.repeat(
        keys[0].reshape(token_row_block, KEY_VALUE_HEADS, HEAD_CHANNELS), group_copies, axis=1
    ).reshape(token_row_block, key_value_width * group_copies)
    value_positions = jnp.repeat(
        values[0].reshape(token_row_block, KEY_VALUE_HEADS, HEAD_CHANNELS), group_copies, axis=1
    ).reshape(token_row_block, key_value_width * group_copies)
    grad_heads, query_heads, key_heads, value_heads = (
        lax.all_to_all(out_grad[0], "sp", split_axis=1, concat_axis=0, tiled=True),
        lax.all_to_all(queries[0], "sp", split_axis=1, concat_axis=0, tiled=True),
        lax.all_to_all(key_positions, "sp", split_axis=1, concat_axis=0, tiled=True),
        lax.all_to_all(value_positions, "sp", split_axis=1, concat_axis=0, tiled=True),
    )
    cos_tab, sin_tab = rotary_tables(token_length)
    query_part, key_portion, value_portion = head_grads(
        query_heads.reshape(token_length, kv_here, portion_heads, HEAD_CHANNELS),
        key_heads.reshape(token_length, kv_here, HEAD_CHANNELS),
        value_heads.reshape(token_length, kv_here, HEAD_CHANNELS),
        grad_heads.reshape(token_length, kv_here, portion_heads, HEAD_CHANNELS),
        query_gain,
        key_gain,
        cos_tab,
        sin_tab,
        min(512, token_length),
    )
    query_tokens, key_token_rows, value_token_rows = (
        lax.all_to_all(
            query_part.reshape(token_length, local_heads * HEAD_CHANNELS),
            "sp",
            split_axis=0,
            concat_axis=1,
            tiled=True,
        ),
        lax.all_to_all(
            key_portion.reshape(token_length, kv_here * HEAD_CHANNELS),
            "sp",
            split_axis=0,
            concat_axis=1,
            tiled=True,
        ),
        lax.all_to_all(
            value_portion.reshape(token_length, kv_here * HEAD_CHANNELS),
            "sp",
            split_axis=0,
            concat_axis=1,
            tiled=True,
        ),
    )
    key_gradient = (
        key_token_rows.reshape(token_row_block, KEY_VALUE_HEADS, group_copies, HEAD_CHANNELS)
        .astype(jnp.float32)
        .sum(axis=2)
        .astype(jnp.bfloat16)
    )
    value_gradient = (
        value_token_rows.reshape(token_row_block, KEY_VALUE_HEADS, group_copies, HEAD_CHANNELS)
        .astype(jnp.float32)
        .sum(axis=2)
        .astype(jnp.bfloat16)
    )
    projection_gradient = jnp.concatenate(
        [
            key_gradient.reshape(token_row_block, key_value_width),
            value_gradient.reshape(token_row_block, key_value_width),
        ],
        axis=1,
    )
    joined_weight = jnp.concatenate([key_matrix, value_matrix], axis=1)
    input_grad = lax.dot_general(
        projection_gradient,
        lax.all_gather(joined_weight, "dp", axis=0, tiled=True),
        (((1,), (1,)), ((), ())),
        preferred_element_type=jnp.float32,
    ).astype(jnp.bfloat16)
    token_in = inputs[0]
    width = inputs.shape[2]
    row_share = width // (sp_count * dp_count)
    permuted = (
        token_in.reshape(token_row_block, dp_count, sp_count, row_share)
        .transpose(0, 2, 1, 3)
        .reshape(token_row_block, width)
    )
    share_cols = lax.all_to_all(permuted, "sp", split_axis=1, concat_axis=0, tiled=True)
    all_grads = lax.all_gather(projection_gradient, "sp", axis=0, tiled=True)
    grad_piece = lax.psum_scatter(
        lax.dot_general(
            share_cols, all_grads, (((0,), (0,)), ((), ())), preferred_element_type=jnp.float32
        ).astype(jnp.bfloat16),
        "dp",
        scatter_dimension=0,
        tiled=True,
    ).astype(jnp.float32)
    weight_grad = lax.all_gather(grad_piece, "sp", axis=0, tiled=True)
    return (
        input_grad[None],
        query_tokens[None],
        weight_grad[:, :key_value_width],
        weight_grad[:, key_value_width:],
    )


LANES = 128
VMEM_BYTES = 67043328
MESH = pl.DeviceIdType.MESH
F32 = jnp.float32
BF16 = jnp.bfloat16


def pair_tables(token_length):
    position = np.arange(token_length)
    half_pairs = HEAD_CHANNELS // 4
    inv_freq = (rope_base ** (-np.arange(half_pairs) / half_pairs)).astype(np.float32)
    row = (position // GRID).astype(np.float32)
    col = (position % GRID).astype(np.float32)
    angles = np.concatenate([row[:, None] * inv_freq, col[:, None] * inv_freq], axis=1)
    cos_tab = np.repeat(np.cos(angles), 2, axis=1)
    sin_tab = np.repeat(np.sin(angles), 2, axis=1)
    sin_tab[:, 0::2] *= -1.0
    return (
        np.tile(cos_tab, (1, 2)).astype(np.float32),
        np.tile(sin_tab, (1, 2)).astype(np.float32),
    )


def swap_pairs(x):
    lane = lax.broadcasted_iota(jnp.int32, x.shape, 1)
    return jnp.where(lane % 2 == 0, pltpu.roll(x, LANES - 1, 1), pltpu.roll(x, 1, 1))


def head_mean(z):
    row = lax.broadcasted_iota(jnp.int32, (LANES, LANES), 0) // HEAD_CHANNELS
    col = lax.broadcasted_iota(jnp.int32, (LANES, LANES), 1) // HEAD_CHANNELS
    ones = jnp.where(row == col, 1.0, 0.0).astype(BF16)
    high = z.astype(BF16)
    low = (z - high.astype(F32)).astype(BF16)
    total = jnp.dot(high, ones, preferred_element_type=F32)
    total = total + jnp.dot(low, ones, preferred_element_type=F32)
    return total * (1.0 / HEAD_CHANNELS)


def norm_rotate(x, gain, cos_tab, sin_tab):
    inv = lax.rsqrt(head_mean(x * x) + norm_eps)
    y = x * inv * gain
    return y * cos_tab + swap_pairs(y) * sin_tab


def norm_rotate_back(x, cotangent, gain, cos_tab, sin_tab):
    turned = cotangent * cos_tab - swap_pairs(cotangent) * sin_tab
    inv = lax.rsqrt(head_mean(x * x) + norm_eps)
    weighted = turned * gain
    return inv * (weighted - x * (inv * inv * head_mean(weighted * x)))


def contract(a, b, dims):
    return lax.dot_general(a, b, (dims, ((), ())), preferred_element_type=F32)


def step_kernel(
    n, dp,
    x_hbm, q_hbm, k_hbm, v_hbm, do_hbm, qg_hbm, kg_hbm, km_hbm, vm_hbm, cos_hbm, sin_hbm,
    dx_buf, dq_buf, kw_buf, vw_buf,
    qg_ref, kg_ref, q_buf, do_buf, cos_buf, sin_buf, k_all, v_all, x_all, wk_all, wv_all,
    q_st, do_st, k_st, v_st, dq_acc, part, got, far, g_all, x_t, wg_part, wg_got,
    fin_all,
    local_sem, kv_send, kv_recv, x_send, x_recv, w_send, w_recv, w_fsend,
    kv_fsend, far_send, far_recv, p_send, p_recv, g_send, g_recv, g_fsend, r_send, r_recv, f_send, f_recv,
):
    me = lax.axis_index("sp")
    md = lax.axis_index("dp")
    rows, q_width = q_buf.shape
    head_pairs = k_all.shape[0]
    share = x_all.shape[2]
    per_group = q_width // (2 * head_pairs * HEAD_CHANNELS)
    mate = md + 1 - 2 * (md % 2)
    piece = share // n

    def sp_peer(o):
        return lax.rem(me + o, n)

    def sp_from(o):
        return lax.rem(me - o + n, n)

    def dp_peer(o):
        return lax.rem(md + o, dp)

    def dp_from(o):
        return lax.rem(md - o + dp, dp)

    def mate_from(o):
        return lax.rem(mate - o + dp, dp)

    def pair(c):
        return pl.ds(c * LANES, LANES)

    barrier = pltpu.get_barrier_semaphore()
    for o in range(1, n):
        pl.semaphore_signal(barrier, inc=1, device_id={"sp": sp_peer(o)}, device_id_type=MESH)
    for o in range(1, dp):
        pl.semaphore_signal(barrier, inc=1, device_id={"dp": dp_peer(o)}, device_id_type=MESH)

    def columns(d):
        return pl.ds(pl.multiple_of(d * share, share), share)

    wanted = [
        (q_hbm, q_buf), (do_hbm, do_buf), (cos_hbm, cos_buf), (sin_hbm, sin_buf),
        (x_hbm.at[:, columns(md)], x_all.at[md]),
        (km_hbm, wk_all.at[md]), (vm_hbm, wv_all.at[md]), (qg_hbm, qg_ref), (kg_hbm, kg_ref),
    ]
    for c in range(head_pairs):
        wanted.append((k_hbm.at[:, pair(c)], k_all.at[c, me]))
        wanted.append((v_hbm.at[:, pair(c)], v_all.at[c, me]))
    local = [
        pltpu.make_async_copy(src, dst, local_sem.at[i]) for i, (src, dst) in enumerate(wanted)
    ]
    for copy in local:
        copy.start()

    def remote(src, dst, send, recv, where):
        return pltpu.make_async_remote_copy(
            src_ref=src, dst_ref=dst, send_sem=send, recv_sem=recv,
            device_id=where, device_id_type=MESH,
        )

    pl.semaphore_wait(barrier, n + dp - 2)

    sends = []

    def only_if(condition, act):
        if condition is None:
            act()
        else:
            pl.when(condition)(act)

    def send(*args, condition=None):
        copy = remote(*args)
        only_if(condition, copy.start)
        sends.append((condition, copy))

    def arrived(dst, recv):
        remote(dst, dst, recv, recv, {"sp": me}).wait_recv()

    line = n == 4
    near_right = {1: me != n - 1, n - 1: me != 0} if line else {}
    near_left = {1: me != 0, n - 1: me != n - 1} if line else {}
    inner = (me != 0) & (me != n - 1)
    outer = (me == 0) | (me == n - 1)
    inward = jnp.where(me == 0, 1, n - 2)
    order = sorted(range(1, n), key=lambda o: -min(o, n - o))
    for c in range(head_pairs):
        for kind, (src, dst) in enumerate([(k_hbm, k_all), (v_hbm, v_all)]):
            for o in order:
                send(src.at[:, pair(c)], dst.at[c, me], kv_send.at[kind, c, o],
                     kv_recv.at[kind, c, me], {"sp": sp_peer(o)}, condition=near_right.get(o))
    weights = [(km_hbm, wk_all), (vm_hbm, wv_all)]
    for kind, (src, dst) in enumerate(weights):
        for o in range(2, dp, 2):
            send(src, dst.at[md], w_send.at[kind, o], w_recv.at[kind, md], {"dp": dp_peer(o)})
        send(src, dst.at[md], w_send.at[kind, 1], w_recv.at[kind, md], {"dp": mate})
    for o in range(1, dp):
        send(x_hbm.at[:, columns(dp_peer(o))], x_all.at[md], x_send.at[o], x_recv.at[md],
             {"dp": dp_peer(o)})

    for copy in local:
        copy.wait()

    my_rows = pl.ds(pl.multiple_of(me * rows, rows), rows)
    cos_own = cos_buf[my_rows, :]
    sin_own = sin_buf[my_rows, :]
    q_gain = jnp.concatenate([qg_ref[...], qg_ref[...]], axis=1)
    k_gain = jnp.concatenate([kg_ref[...], kg_ref[...]], axis=1)

    for c in range(q_width // LANES):
        turned = norm_rotate(q_buf[:, pair(c)].astype(F32), q_gain, cos_own, sin_own).astype(BF16)
        grads = do_buf[:, pair(c)]
        for a in range(2):
            h = 2 * c + a
            to = pl.ds((h % per_group) * rows, rows)
            half = slice(a * HEAD_CHANNELS, (a + 1) * HEAD_CHANNELS)
            q_st[h // per_group, to, :] = turned[:, half]
            do_st[h // per_group, to, :] = grads[:, half]

    def stack_keys(c, src):
        at = pl.ds(pl.multiple_of(src * rows, rows), rows)
        turned = norm_rotate(
            k_all[c, src].astype(F32), k_gain, cos_buf[at, :], sin_buf[at, :]
        ).astype(BF16)
        vals = v_all[c, src]
        for a in range(2):
            half = slice(a * HEAD_CHANNELS, (a + 1) * HEAD_CHANNELS)
            k_st[2 * c + a, at, :] = turned[:, half]
            v_st[2 * c + a, at, :] = vals[:, half]

    def attend(g):
        qs = q_st[g]
        dos = do_st[g]
        ks = k_st[g]
        vs = v_st[g]
        scores = contract(ks, qs, ((1,), (1,))) * score_scale
        shifted = jnp.exp(scores - jnp.max(scores, axis=0, keepdims=True))
        prob = shifted * (1.0 / jnp.sum(shifted, axis=0, keepdims=True))
        value_part = contract(prob.astype(BF16), dos, ((1,), (0,)))
        prob_grad = contract(vs, dos, ((1,), (1,)))
        row_dot = jnp.sum(prob * prob_grad, axis=0, keepdims=True)
        score_grad = (prob * (prob_grad - row_dot) * score_scale).astype(BF16)
        key_part = contract(score_grad, qs, ((1,), (0,)))
        dq_t = contract(ks, score_grad, ((0,), (0,)))
        for r in range(0, per_group, 2):
            both = jnp.concatenate(
                [dq_t[:, r * rows:(r + 1) * rows], dq_t[:, (r + 1) * rows:(r + 2) * rows]], axis=0
            )
            head = g * per_group + r
            dq_acc[:, head * HEAD_CHANNELS:head * HEAD_CHANNELS + LANES] = both.T
        return key_part, value_part

    def add_far(c):
        if not line:
            return
        across = sp_peer(2)
        copy = remote(part.at[c, across], got.at[c, me], p_send.at[c, 2], p_recv.at[c, me],
                      {"sp": across})

        @pl.when(inner)
        def _():
            arrived(far.at[c], far_recv.at[c])
            part[c, across] = (part[c, across].astype(F32) + far[c].astype(F32)).astype(BF16)
            copy.start()

        sends.append((inner, copy))

    if line:
        @pl.when(outer)
        def _():
            for c in range(head_pairs):
                got[c, n - 1 - me] = jnp.zeros(got.shape[2:], BF16)

    for c in range(head_pairs):
        stack_keys(c, me)
    for c in range(head_pairs):
        for o in order:
            src = sp_from(o)
            for kind, ref in enumerate([k_all, v_all]):
                arrived(ref.at[c, src], kv_recv.at[kind, c, src])
                if line and o == 2:
                    send(ref.at[c, src], ref.at[c, src], kv_fsend.at[kind, c],
                         kv_recv.at[kind, c, src], {"sp": jnp.where(me == 1, 0, n - 1)},
                         condition=inner)
            stack_keys(c, src)
        if c:
            add_far(c - 1)
        key_low, value_low = attend(2 * c)
        key_high, value_high = attend(2 * c + 1)
        both = jnp.concatenate([key_low, key_high, value_low, value_high], axis=1).astype(BF16)
        for j in range(n):
            part[c, j] = both[j * rows:(j + 1) * rows, :]
        if line:
            send(part.at[c, n - 1 - me], far.at[c], far_send.at[c], far_recv.at[c],
                 {"sp": inward}, condition=outer)
        for o in order:
            send(part.at[c, sp_peer(o)], got.at[c, me], p_send.at[c, o], p_recv.at[c, me],
                 {"sp": sp_peer(o)}, condition=outer if line and o == 2 else near_right.get(o))
    add_far(head_pairs - 1)

    def own_grads(c):
        total = part[c, me].astype(F32)
        for o in range(1, n):
            src = sp_from(o)
            only_if(near_left.get(o), functools.partial(arrived, got.at[c, src], p_recv.at[c, src]))
            total = total + got[c, src].astype(F32)
        g_all[c, md, :, :LANES] = norm_rotate_back(
            k_all[c, me].astype(F32), total[:, :LANES], k_gain, cos_own, sin_own
        ).astype(BF16)
        g_all[c, md, :, LANES:] = total[:, LANES:].astype(BF16)
        mine = g_all.at[c, md]
        for o in range(2, dp, 2):
            send(mine, mine, g_send.at[c, o], g_recv.at[c, md], {"dp": dp_peer(o)})
        send(mine, mine, g_send.at[c, 1], g_recv.at[c, md], {"dp": mate})

    def pass_on(c):
        for o in range(2, dp, 2):
            src = dp_from(o)
            theirs = g_all.at[c, src]
            arrived(theirs, g_recv.at[c, src])
            send(theirs, theirs, g_fsend.at[c, o], g_recv.at[c, src], {"dp": mate})

    def weight_grads(c):
        total = contract(x_t[md], g_all[c, md], ((1,), (0,)))
        for o in range(2, dp, 2):
            src = dp_from(o)
            total = total + contract(x_t[src], g_all[c, src], ((1,), (0,)))
        for o in range(0, dp, 2):
            src = mate_from(o)
            arrived(g_all.at[c, src], g_recv.at[c, src])
            total = total + contract(x_t[src], g_all[c, src], ((1,), (0,)))
        for j in range(n):
            wg_part[c, j] = total[j * piece:(j + 1) * piece, :].astype(BF16)
        for o in order:
            send(wg_part.at[c, sp_peer(o)], wg_got.at[c, me], r_send.at[c, o], r_recv.at[c, me],
                 {"sp": sp_peer(o)})

    def sum_weight_grads(c):
        total = wg_part[c, me].astype(F32)
        for o in range(1, n):
            src = sp_from(o)
            arrived(wg_got.at[c, src], r_recv.at[c, src])
            total = total + wg_got[c, src].astype(F32)
        fin_all[c, me] = total.astype(BF16)
        mine = fin_all.at[c, me]
        for o in order:
            send(mine, mine, f_send.at[c, o], f_recv.at[c, me], {"sp": sp_peer(o)})

    for o in range(dp):
        src = dp_from(o)
        if o:
            arrived(x_all.at[src], x_recv.at[src])
        x_t[src] = x_all[src].T

    for c in range(head_pairs):
        own_grads(c)
        if c == 0:
            for kind, (_, dst) in enumerate(weights):
                for o in range(2, dp, 2):
                    src = dp_from(o)
                    arrived(dst.at[src], w_recv.at[kind, src])
                    send(dst.at[src], dst.at[src], w_fsend.at[kind, o], w_recv.at[kind, src],
                         {"dp": mate})
            for i in range(q_width // LANES):
                dq_buf[:, pair(i)] = norm_rotate_back(
                    q_buf[:, pair(i)].astype(F32), dq_acc[:, pair(i)], q_gain, cos_own, sin_own
                ).astype(BF16)

    own = jnp.concatenate(
        [g_all[c, md, :, :LANES] for c in range(head_pairs)]
        + [g_all[c, md, :, LANES:] for c in range(head_pairs)], axis=1)
    kv_width = head_pairs * LANES

    def project(src):
        out = contract(own[:, :kv_width], wk_all[src], ((1,), (1,)))
        out = out + contract(own[:, kv_width:], wv_all[src], ((1,), (1,)))
        dx_buf[:, columns(src)] = out.astype(BF16)

    for c in range(head_pairs):
        pass_on(c)
        weight_grads(c)
    for o in range(0, dp, 2):
        project(dp_from(o))
    for o in range(0, dp, 2):
        src = mate_from(o)
        for kind, (_, dst) in enumerate(weights):
            arrived(dst.at[src], w_recv.at[kind, src])
        project(src)
    for c in range(head_pairs):
        sum_weight_grads(c)
    for c in range(head_pairs):
        for o in range(n):
            src = sp_from(o)
            if o:
                arrived(fin_all.at[c, src], f_recv.at[c, src])
            at = pl.ds(pl.multiple_of(src * piece, piece), piece)
            kw_buf[at, pair(c)] = fin_all[c, src, :, :LANES].astype(F32)
            vw_buf[at, pair(c)] = fin_all[c, src, :, LANES:].astype(F32)
    for condition, copy in sends:
        only_if(condition, copy.wait_send)


def write_kernel(*refs):
    count = (len(refs) - 1) // 2
    copies = [
        pltpu.make_async_copy(refs[i], refs[count + i], refs[-1].at[i]) for i in range(count)
    ]
    for copy in copies:
        copy.start()
    for copy in copies:
        copy.wait()


def kernel_step(
    n, dp, inputs, queries, keys, values, out_grad, query_gain, key_gain, key_matrix, value_matrix
):
    rows, width = inputs.shape[1:]
    q_width = queries.shape[2]
    kv_width = keys.shape[2]
    length = rows * n
    share = width // dp
    kv_heads = kv_width // HEAD_CHANNELS
    half = kv_heads // 2
    stack = rows * (q_width // kv_width)
    cos_tab, sin_tab = pair_tables(length)
    vmem = pltpu.VMEM
    dma = pltpu.SemaphoreType.DMA
    wide = 2 * LANES
    scratch = [
        vmem((1, HEAD_CHANNELS), F32), vmem((1, HEAD_CHANNELS), F32),
        vmem((rows, q_width), BF16), vmem((rows, q_width), BF16),
        vmem((length, LANES), F32), vmem((length, LANES), F32),
        vmem((half, n, rows, LANES), BF16), vmem((half, n, rows, LANES), BF16),
        vmem((dp, rows, share), BF16),
        vmem((dp, share, kv_width), BF16), vmem((dp, share, kv_width), BF16),
        vmem((kv_heads, stack, HEAD_CHANNELS), BF16), vmem((kv_heads, stack, HEAD_CHANNELS), BF16),
        vmem((kv_heads, length, HEAD_CHANNELS), BF16), vmem((kv_heads, length, HEAD_CHANNELS), BF16),
        vmem((rows, q_width), F32),
        vmem((half, n, rows, wide), BF16), vmem((half, n, rows, wide), BF16),
        vmem((half, rows, wide), BF16),
        vmem((half, dp, rows, wide), BF16), vmem((dp, share, rows), BF16),
        vmem((half, n, share // n, wide), BF16), vmem((half, n, share // n, wide), BF16),
        vmem((half, n, share // n, wide), BF16),
        dma((9 + 2 * half,)),
        dma((2, half, n)), dma((2, half, n)), dma((dp,)), dma((dp,)),
        dma((2, dp)), dma((2, dp)), dma((2, dp)),
        dma((2, half)), dma((half,)), dma((half,)),
        dma((half, n)), dma((half, n)),
        dma((half, dp)), dma((half, dp)), dma((half, dp)),
        dma((half, n)), dma((half, n)), dma((half, n)), dma((half, n)),
    ]
    hbm = pl.BlockSpec(memory_space=pltpu.HBM)
    here = pl.BlockSpec(memory_space=pltpu.VMEM)
    results = [
        ((rows, width), BF16), ((rows, q_width), BF16),
        ((share, kv_width), F32), ((share, kv_width), F32),
    ]
    held_bytes = 65536 + sum(a * b * jnp.dtype(kind).itemsize for (a, b), kind in results)
    held = pl.pallas_call(
        functools.partial(step_kernel, n, dp),
        out_shape=[pltpu.VMEM(shape, kind) for shape, kind in results],
        in_specs=[hbm] * 11,
        out_specs=[here] * 4,
        scratch_shapes=scratch,
        compiler_params=pltpu.CompilerParams(
            collective_id=0, has_side_effects=True, vmem_limit_bytes=VMEM_BYTES - held_bytes
        ),
    )(
        inputs[0], queries[0], keys[0], values[0], out_grad[0],
        query_gain[None], key_gain[None],
        key_matrix, value_matrix, jnp.asarray(cos_tab), jnp.asarray(sin_tab),
    )
    dx, dq, kw, vw = pl.pallas_call(
        write_kernel,
        out_shape=[jax.ShapeDtypeStruct(shape, kind) for shape, kind in results],
        in_specs=[here] * 4,
        out_specs=[hbm] * 4,
        scratch_shapes=[dma((4,))],
        compiler_params=pltpu.CompilerParams(vmem_limit_bytes=8 * 1024 * 1024),
    )(*held)
    return dx[None], dq[None], kw, vw


def device_step(inputs, *rest):
    n = lax.axis_size("sp")
    dp = lax.axis_size("dp")
    rows, width = inputs.shape[1:]
    fits = dp % 2 == 0 and width % (dp * LANES) == 0 and rows % LANES == 0 and rows * n <= 1024
    if fits and (width // dp) % (16 * n) == 0:
        return kernel_step(n, dp, inputs, *rest)
    return on_device(inputs, *rest)


def solution(mesh):
    return jax.shard_map(
        device_step,
        mesh=mesh,
        in_specs=(
            P("dp", "sp", None),
            P("dp", "sp", None),
            P("dp", "sp", None),
            P("dp", "sp", None),
            P("dp", "sp", None),
            P(),
            P(),
            P("dp", None),
            P("dp", None),
        ),
        out_specs=(P("dp", "sp", None), P("dp", "sp", None), P("dp", None), P("dp", None)),
        check_vma=False,
    )
```

```python
import functools

import jax
import jax.numpy as jnp
import numpy as np
from jax import lax
from jax.experimental import pallas as pl
from jax.experimental.pallas import tpu as pltpu
from jax.sharding import PartitionSpec as P

QUERY_HEADS = 16
KEY_VALUE_HEADS = 4
HEAD_CHANNELS = 64
GRID = 64


rope_base = 10000.0
norm_eps = 0.5
score_scale = 0.125


def product(pattern, first_op, second_op):
    return jnp.einsum(pattern, first_op, second_op, preferred_element_type=jnp.float32)


def rotary_tables(token_length):
    position = jnp.arange(token_length, dtype=jnp.int32)
    grid_row = (position // GRID).astype(jnp.float32)
    grid_col = (position % GRID).astype(jnp.float32)
    half_pairs = HEAD_CHANNELS // 4
    inv_freq = rope_base ** (-jnp.arange(half_pairs, dtype=jnp.float32) / half_pairs)
    angles = jnp.concatenate([grid_row[:, None] * inv_freq, grid_col[:, None] * inv_freq], axis=1)
    return (jnp.cos(angles), jnp.sin(angles))


def rotate(vector, cos_tab, sin_tab):
    even_part = vector[..., 0::2]
    odd_part = vector[..., 1::2]
    turned = jnp.stack(
        [even_part * cos_tab - odd_part * sin_tab, even_part * sin_tab + odd_part * cos_tab],
        axis=-1,
    )
    return turned.reshape(vector.shape)


def rotate_back(cotangent, cos_tab, sin_tab):
    even_part = cotangent[..., 0::2]
    odd_part = cotangent[..., 1::2]
    turned = jnp.stack(
        [even_part * cos_tab + odd_part * sin_tab, odd_part * cos_tab - even_part * sin_tab],
        axis=-1,
    )
    return turned.reshape(cotangent.shape)


def inverse_rms(vector):
    return lax.rsqrt(jnp.mean(vector * vector, axis=-1, keepdims=True) + norm_eps)


def norm_back(vector, inv_scale, cotangent, gain_vec):
    weighted = cotangent * gain_vec
    inner_mean = jnp.mean(weighted * vector, axis=-1, keepdims=True)
    return inv_scale * (weighted - vector * inv_scale * inv_scale * inner_mean)


def head_grads(
    query_in, key_input, value_input, grad_in, query_gain, key_gain, cos_tab, sin_tab, block_rows
):
    token_length, groups, per_group, head_dim = query_in.shape
    cos_four = cos_tab[:, None, None, :]
    sin_four = sin_tab[:, None, None, :]
    cos_three = cos_tab[:, None, :]
    sin_three = sin_tab[:, None, :]
    query_f = query_in.astype(jnp.float32)
    query_inv = inverse_rms(query_f)
    query_rot = rotate(query_f * query_inv * query_gain, cos_four, sin_four).astype(jnp.bfloat16)
    key_f = key_input.astype(jnp.float32)
    key_inv = inverse_rms(key_f)
    key_rot = rotate(key_f * key_inv * key_gain, cos_three, sin_three).astype(jnp.bfloat16)
    num_blocks = token_length // block_rows
    query_blocks = query_rot.reshape(num_blocks, block_rows, groups, per_group, head_dim)
    grad_blocks = grad_in.reshape(num_blocks, block_rows, groups, per_group, head_dim)

    def attend_block(carried, pieces):
        key_acc, value_acc = carried
        query_piece, grad_piece = pieces
        scores = product("qgrd,cgd->grqc", query_piece, key_rot) * score_scale
        row_max = jnp.max(scores, axis=-1, keepdims=True)
        shifted = jnp.exp(scores - row_max)
        attn_prob = shifted / jnp.sum(shifted, axis=-1, keepdims=True)
        prob_low = attn_prob.astype(jnp.bfloat16)
        prob_grad = product("qgrd,cgd->grqc", grad_piece, value_input)
        row_dot = jnp.sum(attn_prob * prob_grad, axis=-1, keepdims=True)
        score_grad = (attn_prob * (prob_grad - row_dot) * score_scale).astype(jnp.bfloat16)
        dq_piece = product("grqc,cgd->qgrd", score_grad, key_rot)
        key_acc = key_acc + product("grqc,qgrd->cgd", score_grad, query_piece)
        value_acc = value_acc + product("grqc,qgrd->cgd", prob_low, grad_piece)
        return ((key_acc, value_acc), dq_piece)

    empty_acc = jnp.zeros((token_length, groups, head_dim), jnp.float32)
    (key_rot_grad, value_acc), query_rot_grad = lax.scan(
        attend_block, (empty_acc, empty_acc), (query_blocks, grad_blocks)
    )
    query_rot_grad = query_rot_grad.reshape(token_length, groups, per_group, head_dim)
    query_grad = norm_back(
        query_f, query_inv, rotate_back(query_rot_grad, cos_four, sin_four), query_gain
    ).astype(jnp.bfloat16)
    key_portion = norm_back(
        key_f, key_inv, rotate_back(key_rot_grad, cos_three, sin_three), key_gain
    ).astype(jnp.bfloat16)
    return (query_grad, key_portion, value_acc.astype(jnp.bfloat16))


def on_device(
    inputs, queries, keys, values, out_grad, query_gain, key_gain, key_matrix, value_matrix
):
    sp_count = lax.axis_size("sp")
    dp_count = lax.axis_size("dp")
    token_row_block = inputs.shape[1]
    token_length = token_row_block * sp_count
    local_heads = QUERY_HEADS // sp_count
    portion_heads = min(local_heads, QUERY_HEADS // KEY_VALUE_HEADS)
    kv_here = local_heads // portion_heads
    group_copies = QUERY_HEADS // KEY_VALUE_HEADS // portion_heads
    key_value_width = KEY_VALUE_HEADS * HEAD_CHANNELS
    key_positions = jnp.repeat(
        keys[0].reshape(token_row_block, KEY_VALUE_HEADS, HEAD_CHANNELS), group_copies, axis=1
    ).reshape(token_row_block, key_value_width * group_copies)
    value_positions = jnp.repeat(
        values[0].reshape(token_row_block, KEY_VALUE_HEADS, HEAD_CHANNELS), group_copies, axis=1
    ).reshape(token_row_block, key_value_width * group_copies)
    grad_heads, query_heads, key_heads, value_heads = (
        lax.all_to_all(out_grad[0], "sp", split_axis=1, concat_axis=0, tiled=True),
        lax.all_to_all(queries[0], "sp", split_axis=1, concat_axis=0, tiled=True),
        lax.all_to_all(key_positions, "sp", split_axis=1, concat_axis=0, tiled=True),
        lax.all_to_all(value_positions, "sp", split_axis=1, concat_axis=0, tiled=True),
    )
    cos_tab, sin_tab = rotary_tables(token_length)
    query_part, key_portion, value_portion = head_grads(
        query_heads.reshape(token_length, kv_here, portion_heads, HEAD_CHANNELS),
        key_heads.reshape(token_length, kv_here, HEAD_CHANNELS),
        value_heads.reshape(token_length, kv_here, HEAD_CHANNELS),
        grad_heads.reshape(token_length, kv_here, portion_heads, HEAD_CHANNELS),
        query_gain,
        key_gain,
        cos_tab,
        sin_tab,
        min(512, token_length),
    )
    query_tokens, key_token_rows, value_token_rows = (
        lax.all_to_all(
            query_part.reshape(token_length, local_heads * HEAD_CHANNELS),
            "sp",
            split_axis=0,
            concat_axis=1,
            tiled=True,
        ),
        lax.all_to_all(
            key_portion.reshape(token_length, kv_here * HEAD_CHANNELS),
            "sp",
            split_axis=0,
            concat_axis=1,
            tiled=True,
        ),
        lax.all_to_all(
            value_portion.reshape(token_length, kv_here * HEAD_CHANNELS),
            "sp",
            split_axis=0,
            concat_axis=1,
            tiled=True,
        ),
    )
    key_gradient = (
        key_token_rows.reshape(token_row_block, KEY_VALUE_HEADS, group_copies, HEAD_CHANNELS)
        .astype(jnp.float32)
        .sum(axis=2)
        .astype(jnp.bfloat16)
    )
    value_gradient = (
        value_token_rows.reshape(token_row_block, KEY_VALUE_HEADS, group_copies, HEAD_CHANNELS)
        .astype(jnp.float32)
        .sum(axis=2)
        .astype(jnp.bfloat16)
    )
    projection_gradient = jnp.concatenate(
        [
            key_gradient.reshape(token_row_block, key_value_width),
            value_gradient.reshape(token_row_block, key_value_width),
        ],
        axis=1,
    )
    joined_weight = jnp.concatenate([key_matrix, value_matrix], axis=1)
    input_grad = lax.dot_general(
        projection_gradient,
        lax.all_gather(joined_weight, "dp", axis=0, tiled=True),
        (((1,), (1,)), ((), ())),
        preferred_element_type=jnp.float32,
    ).astype(jnp.bfloat16)
    token_in = inputs[0]
    width = inputs.shape[2]
    row_share = width // (sp_count * dp_count)
    permuted = (
        token_in.reshape(token_row_block, dp_count, sp_count, row_share)
        .transpose(0, 2, 1, 3)
        .reshape(token_row_block, width)
    )
    share_cols = lax.all_to_all(permuted, "sp", split_axis=1, concat_axis=0, tiled=True)
    all_grads = lax.all_gather(projection_gradient, "sp", axis=0, tiled=True)
    grad_piece = lax.psum_scatter(
        lax.dot_general(
            share_cols, all_grads, (((0,), (0,)), ((), ())), preferred_element_type=jnp.float32
        ).astype(jnp.bfloat16),
        "dp",
        scatter_dimension=0,
        tiled=True,
    ).astype(jnp.float32)
    weight_grad = lax.all_gather(grad_piece, "sp", axis=0, tiled=True)
    return (
        input_grad[None],
        query_tokens[None],
        weight_grad[:, :key_value_width],
        weight_grad[:, key_value_width:],
    )


LANES = 128
VMEM_BYTES = 67043328
MESH = pl.DeviceIdType.MESH
F32 = jnp.float32
BF16 = jnp.bfloat16


def pair_tables(token_length):
    position = np.arange(token_length)
    half_pairs = HEAD_CHANNELS // 4
    inv_freq = (rope_base ** (-np.arange(half_pairs) / half_pairs)).astype(np.float32)
    row = (position // GRID).astype(np.float32)
    col = (position % GRID).astype(np.float32)
    angles = np.concatenate([row[:, None] * inv_freq, col[:, None] * inv_freq], axis=1)
    cos_tab = np.repeat(np.cos(angles), 2, axis=1)
    sin_tab = np.repeat(np.sin(angles), 2, axis=1)
    sin_tab[:, 0::2] *= -1.0
    return (
        np.tile(cos_tab, (1, 2)).astype(np.float32),
        np.tile(sin_tab, (1, 2)).astype(np.float32),
    )


def swap_pairs(x):
    lane = lax.broadcasted_iota(jnp.int32, x.shape, 1)
    return jnp.where(lane % 2 == 0, pltpu.roll(x, LANES - 1, 1), pltpu.roll(x, 1, 1))


def head_mean(z):
    row = lax.broadcasted_iota(jnp.int32, (LANES, LANES), 0) // HEAD_CHANNELS
    col = lax.broadcasted_iota(jnp.int32, (LANES, LANES), 1) // HEAD_CHANNELS
    ones = jnp.where(row == col, 1.0, 0.0).astype(BF16)
    high = z.astype(BF16)
    low = (z - high.astype(F32)).astype(BF16)
    total = jnp.dot(high, ones, preferred_element_type=F32)
    total = total + jnp.dot(low, ones, preferred_element_type=F32)
    return total * (1.0 / HEAD_CHANNELS)


def norm_rotate(x, gain, cos_tab, sin_tab):
    inv = lax.rsqrt(head_mean(x * x) + norm_eps)
    y = x * inv * gain
    return y * cos_tab + swap_pairs(y) * sin_tab


def norm_rotate_back(x, cotangent, gain, cos_tab, sin_tab):
    turned = cotangent * cos_tab - swap_pairs(cotangent) * sin_tab
    inv = lax.rsqrt(head_mean(x * x) + norm_eps)
    weighted = turned * gain
    return inv * (weighted - x * (inv * inv * head_mean(weighted * x)))


def contract(a, b, dims):
    return lax.dot_general(a, b, (dims, ((), ())), preferred_element_type=F32)


def step_kernel(
    n, dp,
    x_hbm, q_hbm, k_hbm, v_hbm, do_hbm, qg_hbm, kg_hbm, km_hbm, vm_hbm, cos_hbm, sin_hbm,
    dx_buf, dq_buf, kw_buf, vw_buf,
    qg_ref, kg_ref, q_buf, do_buf, cos_buf, sin_buf, k_all, v_all, x_all, wk_all, wv_all,
    q_st, do_st, k_st, v_st, dq_acc, part, got, g_all, x_t, wg_part, wg_got,
    fin_all,
    local_sem, kv_send, kv_recv, x_send, x_recv, w_send, w_recv, w_fsend,
    p_send, p_recv, g_send, g_recv, g_fsend, r_send, r_recv, f_send, f_recv,
):
    me = lax.axis_index("sp")
    md = lax.axis_index("dp")
    rows, q_width = q_buf.shape
    head_pairs = k_all.shape[0]
    share = x_all.shape[2]
    per_group = q_width // (2 * head_pairs * HEAD_CHANNELS)
    mate = md + 1 - 2 * (md % 2)
    piece = share // n

    def sp_peer(o):
        return lax.rem(me + o, n)

    def sp_from(o):
        return lax.rem(me - o + n, n)

    def dp_peer(o):
        return lax.rem(md + o, dp)

    def dp_from(o):
        return lax.rem(md - o + dp, dp)

    def mate_from(o):
        return lax.rem(mate - o + dp, dp)

    def pair(c):
        return pl.ds(c * LANES, LANES)

    barrier = pltpu.get_barrier_semaphore()
    for o in range(1, n):
        pl.semaphore_signal(barrier, inc=1, device_id={"sp": sp_peer(o)}, device_id_type=MESH)
    for o in range(1, dp):
        pl.semaphore_signal(barrier, inc=1, device_id={"dp": dp_peer(o)}, device_id_type=MESH)

    def columns(d):
        return pl.ds(pl.multiple_of(d * share, share), share)

    wanted = [
        (q_hbm, q_buf), (do_hbm, do_buf), (cos_hbm, cos_buf), (sin_hbm, sin_buf),
        (x_hbm.at[:, columns(md)], x_all.at[md]),
        (km_hbm, wk_all.at[md]), (vm_hbm, wv_all.at[md]), (qg_hbm, qg_ref), (kg_hbm, kg_ref),
    ]
    for c in range(head_pairs):
        wanted.append((k_hbm.at[:, pair(c)], k_all.at[c, me]))
        wanted.append((v_hbm.at[:, pair(c)], v_all.at[c, me]))
    local = [
        pltpu.make_async_copy(src, dst, local_sem.at[i]) for i, (src, dst) in enumerate(wanted)
    ]
    for copy in local:
        copy.start()

    def remote(src, dst, send, recv, where):
        return pltpu.make_async_remote_copy(
            src_ref=src, dst_ref=dst, send_sem=send, recv_sem=recv,
            device_id=where, device_id_type=MESH,
        )

    pl.semaphore_wait(barrier, n + dp - 2)

    sends = []

    def send(*args):
        copy = remote(*args)
        copy.start()
        sends.append(copy)

    def arrived(dst, recv):
        remote(dst, dst, recv, recv, {"sp": me}).wait_recv()

    order = sorted(range(1, n), key=lambda o: -min(o, n - o))
    for c in range(head_pairs):
        for kind, (src, dst) in enumerate([(k_hbm, k_all), (v_hbm, v_all)]):
            for o in order:
                send(src.at[:, pair(c)], dst.at[c, me], kv_send.at[kind, c, o],
                     kv_recv.at[kind, c, me], {"sp": sp_peer(o)})
    weights = [(km_hbm, wk_all), (vm_hbm, wv_all)]
    for kind, (src, dst) in enumerate(weights):
        for o in range(2, dp, 2):
            send(src, dst.at[md], w_send.at[kind, o], w_recv.at[kind, md], {"dp": dp_peer(o)})
        send(src, dst.at[md], w_send.at[kind, 1], w_recv.at[kind, md], {"dp": mate})
    for o in range(1, dp):
        send(x_hbm.at[:, columns(dp_peer(o))], x_all.at[md], x_send.at[o], x_recv.at[md],
             {"dp": dp_peer(o)})

    for copy in local:
        copy.wait()

    my_rows = pl.ds(pl.multiple_of(me * rows, rows), rows)
    cos_own = cos_buf[my_rows, :]
    sin_own = sin_buf[my_rows, :]
    q_gain = jnp.concatenate([qg_ref[...], qg_ref[...]], axis=1)
    k_gain = jnp.concatenate([kg_ref[...], kg_ref[...]], axis=1)

    for c in range(q_width // LANES):
        turned = norm_rotate(q_buf[:, pair(c)].astype(F32), q_gain, cos_own, sin_own).astype(BF16)
        grads = do_buf[:, pair(c)]
        for a in range(2):
            h = 2 * c + a
            to = pl.ds((h % per_group) * rows, rows)
            half = slice(a * HEAD_CHANNELS, (a + 1) * HEAD_CHANNELS)
            q_st[h // per_group, to, :] = turned[:, half]
            do_st[h // per_group, to, :] = grads[:, half]

    def stack_keys(c, src):
        at = pl.ds(pl.multiple_of(src * rows, rows), rows)
        turned = norm_rotate(
            k_all[c, src].astype(F32), k_gain, cos_buf[at, :], sin_buf[at, :]
        ).astype(BF16)
        vals = v_all[c, src]
        for a in range(2):
            half = slice(a * HEAD_CHANNELS, (a + 1) * HEAD_CHANNELS)
            k_st[2 * c + a, at, :] = turned[:, half]
            v_st[2 * c + a, at, :] = vals[:, half]

    def attend(g):
        qs = q_st[g]
        dos = do_st[g]
        ks = k_st[g]
        vs = v_st[g]
        scores = contract(ks, qs, ((1,), (1,))) * score_scale
        shifted = jnp.exp(scores - jnp.max(scores, axis=0, keepdims=True))
        prob = shifted * (1.0 / jnp.sum(shifted, axis=0, keepdims=True))
        value_part = contract(prob.astype(BF16), dos, ((1,), (0,)))
        prob_grad = contract(vs, dos, ((1,), (1,)))
        row_dot = jnp.sum(prob * prob_grad, axis=0, keepdims=True)
        score_grad = (prob * (prob_grad - row_dot) * score_scale).astype(BF16)
        key_part = contract(score_grad, qs, ((1,), (0,)))
        dq_t = contract(ks, score_grad, ((0,), (0,)))
        for r in range(0, per_group, 2):
            both = jnp.concatenate(
                [dq_t[:, r * rows:(r + 1) * rows], dq_t[:, (r + 1) * rows:(r + 2) * rows]], axis=0
            )
            head = g * per_group + r
            dq_acc[:, head * HEAD_CHANNELS:head * HEAD_CHANNELS + LANES] = both.T
        return key_part, value_part

    for c in range(head_pairs):
        stack_keys(c, me)
    for c in range(head_pairs):
        for o in range(1, n):
            src = sp_from(o)
            arrived(k_all.at[c, src], kv_recv.at[0, c, src])
            arrived(v_all.at[c, src], kv_recv.at[1, c, src])
            stack_keys(c, src)
        key_low, value_low = attend(2 * c)
        key_high, value_high = attend(2 * c + 1)
        both = jnp.concatenate([key_low, key_high, value_low, value_high], axis=1).astype(BF16)
        for j in range(n):
            part[c, j] = both[j * rows:(j + 1) * rows, :]
        for o in order:
            send(part.at[c, sp_peer(o)], got.at[c, me], p_send.at[c, o], p_recv.at[c, me],
                 {"sp": sp_peer(o)})

    def own_grads(c):
        total = part[c, me].astype(F32)
        for o in range(1, n):
            src = sp_from(o)
            arrived(got.at[c, src], p_recv.at[c, src])
            total = total + got[c, src].astype(F32)
        g_all[c, md, :, :LANES] = norm_rotate_back(
            k_all[c, me].astype(F32), total[:, :LANES], k_gain, cos_own, sin_own
        ).astype(BF16)
        g_all[c, md, :, LANES:] = total[:, LANES:].astype(BF16)
        mine = g_all.at[c, md]
        for o in range(2, dp, 2):
            send(mine, mine, g_send.at[c, o], g_recv.at[c, md], {"dp": dp_peer(o)})
        send(mine, mine, g_send.at[c, 1], g_recv.at[c, md], {"dp": mate})

    def pass_on(c):
        for o in range(2, dp, 2):
            src = dp_from(o)
            theirs = g_all.at[c, src]
            arrived(theirs, g_recv.at[c, src])
            send(theirs, theirs, g_fsend.at[c, o], g_recv.at[c, src], {"dp": mate})

    def weight_grads(c):
        total = contract(x_t[md], g_all[c, md], ((1,), (0,)))
        for o in range(2, dp, 2):
            src = dp_from(o)
            total = total + contract(x_t[src], g_all[c, src], ((1,), (0,)))
        for o in range(0, dp, 2):
            src = mate_from(o)
            arrived(g_all.at[c, src], g_recv.at[c, src])
            total = total + contract(x_t[src], g_all[c, src], ((1,), (0,)))
        for j in range(n):
            wg_part[c, j] = total[j * piece:(j + 1) * piece, :].astype(BF16)
        for o in order:
            send(wg_part.at[c, sp_peer(o)], wg_got.at[c, me], r_send.at[c, o], r_recv.at[c, me],
                 {"sp": sp_peer(o)})

    def sum_weight_grads(c):
        total = wg_part[c, me].astype(F32)
        for o in range(1, n):
            src = sp_from(o)
            arrived(wg_got.at[c, src], r_recv.at[c, src])
            total = total + wg_got[c, src].astype(F32)
        fin_all[c, me] = total.astype(BF16)
        mine = fin_all.at[c, me]
        for o in order:
            send(mine, mine, f_send.at[c, o], f_recv.at[c, me], {"sp": sp_peer(o)})

    for o in range(dp):
        src = dp_from(o)
        if o:
            arrived(x_all.at[src], x_recv.at[src])
        x_t[src] = x_all[src].T

    for c in range(head_pairs):
        own_grads(c)
        if c == 0:
            for kind, (_, dst) in enumerate(weights):
                for o in range(2, dp, 2):
                    src = dp_from(o)
                    arrived(dst.at[src], w_recv.at[kind, src])
                    send(dst.at[src], dst.at[src], w_fsend.at[kind, o], w_recv.at[kind, src],
                         {"dp": mate})
            for i in range(q_width // LANES):
                dq_buf[:, pair(i)] = norm_rotate_back(
                    q_buf[:, pair(i)].astype(F32), dq_acc[:, pair(i)], q_gain, cos_own, sin_own
                ).astype(BF16)

    own = jnp.concatenate(
        [g_all[c, md, :, :LANES] for c in range(head_pairs)]
        + [g_all[c, md, :, LANES:] for c in range(head_pairs)], axis=1)
    kv_width = head_pairs * LANES

    def project(src):
        out = contract(own[:, :kv_width], wk_all[src], ((1,), (1,)))
        out = out + contract(own[:, kv_width:], wv_all[src], ((1,), (1,)))
        dx_buf[:, columns(src)] = out.astype(BF16)

    for c in range(head_pairs):
        pass_on(c)
        weight_grads(c)
    for o in range(0, dp, 2):
        project(dp_from(o))
    for o in range(0, dp, 2):
        src = mate_from(o)
        for kind, (_, dst) in enumerate(weights):
            arrived(dst.at[src], w_recv.at[kind, src])
        project(src)
    for c in range(head_pairs):
        sum_weight_grads(c)
    for c in range(head_pairs):
        for o in range(n):
            src = sp_from(o)
            if o:
                arrived(fin_all.at[c, src], f_recv.at[c, src])
            at = pl.ds(pl.multiple_of(src * piece, piece), piece)
            kw_buf[at, pair(c)] = fin_all[c, src, :, :LANES].astype(F32)
            vw_buf[at, pair(c)] = fin_all[c, src, :, LANES:].astype(F32)
    for copy in sends:
        copy.wait_send()


def write_kernel(*refs):
    count = (len(refs) - 1) // 2
    copies = [
        pltpu.make_async_copy(refs[i], refs[count + i], refs[-1].at[i]) for i in range(count)
    ]
    for copy in copies:
        copy.start()
    for copy in copies:
        copy.wait()


def kernel_step(
    n, dp, inputs, queries, keys, values, out_grad, query_gain, key_gain, key_matrix, value_matrix
):
    rows, width = inputs.shape[1:]
    q_width = queries.shape[2]
    kv_width = keys.shape[2]
    length = rows * n
    share = width // dp
    kv_heads = kv_width // HEAD_CHANNELS
    half = kv_heads // 2
    stack = rows * (q_width // kv_width)
    cos_tab, sin_tab = pair_tables(length)
    vmem = pltpu.VMEM
    dma = pltpu.SemaphoreType.DMA
    wide = 2 * LANES
    scratch = [
        vmem((1, HEAD_CHANNELS), F32), vmem((1, HEAD_CHANNELS), F32),
        vmem((rows, q_width), BF16), vmem((rows, q_width), BF16),
        vmem((length, LANES), F32), vmem((length, LANES), F32),
        vmem((half, n, rows, LANES), BF16), vmem((half, n, rows, LANES), BF16),
        vmem((dp, rows, share), BF16),
        vmem((dp, share, kv_width), BF16), vmem((dp, share, kv_width), BF16),
        vmem((kv_heads, stack, HEAD_CHANNELS), BF16), vmem((kv_heads, stack, HEAD_CHANNELS), BF16),
        vmem((kv_heads, length, HEAD_CHANNELS), BF16), vmem((kv_heads, length, HEAD_CHANNELS), BF16),
        vmem((rows, q_width), F32),
        vmem((half, n, rows, wide), BF16), vmem((half, n, rows, wide), BF16),
        vmem((half, dp, rows, wide), BF16), vmem((dp, share, rows), BF16),
        vmem((half, n, share // n, wide), BF16), vmem((half, n, share // n, wide), BF16),
        vmem((half, n, share // n, wide), BF16),
        dma((9 + 2 * half,)),
        dma((2, half, n)), dma((2, half, n)), dma((dp,)), dma((dp,)),
        dma((2, dp)), dma((2, dp)), dma((2, dp)),
        dma((half, n)), dma((half, n)),
        dma((half, dp)), dma((half, dp)), dma((half, dp)),
        dma((half, n)), dma((half, n)), dma((half, n)), dma((half, n)),
    ]
    hbm = pl.BlockSpec(memory_space=pltpu.HBM)
    here = pl.BlockSpec(memory_space=pltpu.VMEM)
    results = [
        ((rows, width), BF16), ((rows, q_width), BF16),
        ((share, kv_width), F32), ((share, kv_width), F32),
    ]
    held_bytes = 65536 + sum(a * b * jnp.dtype(kind).itemsize for (a, b), kind in results)
    held = pl.pallas_call(
        functools.partial(step_kernel, n, dp),
        out_shape=[pltpu.VMEM(shape, kind) for shape, kind in results],
        in_specs=[hbm] * 11,
        out_specs=[here] * 4,
        scratch_shapes=scratch,
        compiler_params=pltpu.CompilerParams(
            collective_id=0, has_side_effects=True, vmem_limit_bytes=VMEM_BYTES - held_bytes
        ),
    )(
        inputs[0], queries[0], keys[0], values[0], out_grad[0],
        query_gain[None], key_gain[None],
        key_matrix, value_matrix, jnp.asarray(cos_tab), jnp.asarray(sin_tab),
    )
    dx, dq, kw, vw = pl.pallas_call(
        write_kernel,
        out_shape=[jax.ShapeDtypeStruct(shape, kind) for shape, kind in results],
        in_specs=[here] * 4,
        out_specs=[hbm] * 4,
        scratch_shapes=[dma((4,))],
        compiler_params=pltpu.CompilerParams(vmem_limit_bytes=8 * 1024 * 1024),
    )(*held)
    return dx[None], dq[None], kw, vw


def device_step(inputs, *rest):
    n = lax.axis_size("sp")
    dp = lax.axis_size("dp")
    rows, width = inputs.shape[1:]
    fits = dp % 2 == 0 and width % (dp * LANES) == 0 and rows % LANES == 0 and rows * n <= 1024
    if fits and (width // dp) % (16 * n) == 0:
        return kernel_step(n, dp, inputs, *rest)
    return on_device(inputs, *rest)


def solution(mesh):
    return jax.shard_map(
        device_step,
        mesh=mesh,
        in_specs=(
            P("dp", "sp", None),
            P("dp", "sp", None),
            P("dp", "sp", None),
            P("dp", "sp", None),
            P("dp", "sp", None),
            P(),
            P(),
            P("dp", None),
            P("dp", None),
        ),
        out_specs=(P("dp", "sp", None), P("dp", "sp", None), P("dp", None), P("dp", None)),
        check_vma=False,
    )
```
